32 devices in a mesh: sp: 8 (over z, y), tp: 4 (over x, core).
Axes of the slice: x: 2, y: 2, z: 4, core: 2. Of those that a mesh axis runs over, the one named last changes fastest.
Arguments:
- mixer_input: bfloat16 [2048, 1024], P('sp', 'tp'), may hold values from -6 to 6
- retention: float32 [64, 2048], P('tp', 'sp'), may hold values from -1 to 0
- decay_real: float32 [64, 64], P('tp'), may hold values from -0.7 to -0.3
- decay_freq: float32 [64, 64], P('tp'), may hold values from 0 to 26
- log_step: float32 [64], P('tp')
- input_real: float32 [64, 64, 16], P('tp')
- input_imag: float32 [64, 64, 16], P('tp')
- readout_real: float32 [64, 16, 64], P('tp'), may hold values from -0.5 to 0.5
- readout_imaginary: float32 [64, 16, 64], P('tp'), may hold values from -0.5 to 0.5
- skip_weight: float32 [64, 16], P('tp'), may hold values from -4 to 4
- norm_gain: float32 [1024], replicated, may hold values from 0.1 to 1.9
- projection: bfloat16 [1024, 2048], P('tp'), may hold values from -0.1875 to 0.1875
- residual: bfloat16 [2048, 2048], P(('sp', 'tp')), may hold values from -6 to 6
- mix_gain: float32 [2048], replicated, may hold values from 0.1 to 1.9
- routes: int32 [2048, 2], P(('sp', 'tp')), may hold values from 0 to 7, all different within a row; in each aligned block of 64 rows (0 to 63, 64 to 127, ...) at most 32 rows name the same one
- route_weight: float32 [2048, 2], P(('sp', 'tp')), may hold values from 0.5 to 2
- expert_gate: bfloat16 [8, 2048, 512], P('sp'), may hold values from -0.125 to 0.125
- expert_up: bfloat16 [8, 2048, 512], P('sp'), may hold values from -0.125 to 0.125
- expert_down: bfloat16 [8, 512, 2048], P('sp'), may hold values from -0.25 to 0.25
- final_gain: float32 [2048], replicated, may hold values from 0.1 to 1.9
Outputs:
- layer_out: bfloat16 [2048, 2048], P(('sp', 'tp'))
The draws below stay inside these ranges and needn't reach their ends.
Inputs may be any that keep to these rules, and one draw needn't show every extreme that they name: `routes`: in each aligned block of 64 rows no expert is named by more than 32 rows, and in some blocks one is named by exactly 32 rows; each row names 2 different experts.
All inputs are finite; a program needn't handle non-finite values.
Results may differ from the reference program's by a relative error of at most 0.017.
Values may be sent and summed in bfloat16 or wider, within the bound.
A program may use at most 64 MiB of HBM per device.

```python
import math
import jax
import jax.numpy as jnp
import numpy as np
from jax import lax

WIDTH = 2048
GROUPS = 64
CHANNELS = 16
STATE = 64
EXPERT_HIDDEN = 512
PICKS = 2
SHARD_TOKENS = 256
MIX_WIDTH = 1024
SEQUENCE_TOKENS = 2048
DEVICE_ROWS = 64
EXPERTS = 8
CAPACITY = 32


def decay_plan(key):
    folded_values = jax.random.fold_in(key, 7)
    slow_share = 0.5
    slow_group = jax.random.uniform(jax.random.fold_in(folded_values, 1), (GROUPS,), jnp.float32) < slow_share
    decay_real = -jax.random.uniform(jax.random.fold_in(folded_values, 2), (GROUPS, STATE), jnp.float32, 0.3, 0.7)
    decay_freq = jax.random.uniform(jax.random.fold_in(folded_values, 3), (GROUPS, STATE), jnp.float32, 0.0, 8.0 * math.pi)
    fast_log = jax.random.uniform(jax.random.fold_in(folded_values, 4), (GROUPS,), jnp.float32, math.log(0.04), math.log(0.12))
    slow_log = jax.random.uniform(jax.random.fold_in(folded_values, 5), (GROUPS,), jnp.float32, math.log(0.2 / SEQUENCE_TOKENS), math.log(0.6 / SEQUENCE_TOKENS))
    log_step = jnp.where(slow_group, slow_log, fast_log)
    stride = jnp.exp(log_step)[:, None]
    growth = decay_real * stride
    turning = decay_freq * stride
    upper_real = jnp.expm1(growth) * jnp.cos(turning) - 2.0 * jnp.sin(0.5 * turning) ** 2
    upper_imag = jnp.exp(growth) * jnp.sin(turning)
    magnitude = jnp.sqrt(upper_real * upper_real + upper_imag * upper_imag)
    magnitude = magnitude / jnp.sqrt(decay_real * decay_real + decay_freq * decay_freq)
    scaling = jnp.sqrt(-2.0 * growth) / magnitude / math.sqrt(CHANNELS)
    return (decay_real, decay_freq, log_step, scaling)


def draw_decay_real(key, part):
    return decay_plan(key)[0]


def draw_decay_freq(key, part):
    return decay_plan(key)[1]


def draw_log_step(key, part):
    return decay_plan(key)[2]


def draw_input_real(key, part):
    scaling = decay_plan(key)[3]
    return scaling[:, :, None] * jax.random.normal(jax.random.fold_in(key, 21), (GROUPS, STATE, CHANNELS), jnp.float32)


def draw_input_imag(key, part):
    scaling = decay_plan(key)[3]
    return scaling[:, :, None] * jax.random.normal(jax.random.fold_in(key, 22), (GROUPS, STATE, CHANNELS), jnp.float32)


def draw_retention(key, part):
    folded_values = jax.random.fold_in(key, 13)
    blocks = SEQUENCE_TOKENS // SHARD_TOKENS
    factor = jnp.exp(jax.random.uniform(jax.random.fold_in(folded_values, 1), (GROUPS, blocks), jnp.float32, 0.0, math.log(4.0)))
    roughness = jax.random.uniform(jax.random.fold_in(folded_values, 2), (GROUPS, SEQUENCE_TOKENS), jnp.float32, 0.5, 1.5)
    base_level = 0.2
    steady_state = -(base_level / SEQUENCE_TOKENS) * jnp.repeat(factor, SHARD_TOKENS, axis=1) * roughness
    spike_locations = jax.random.randint(jax.random.fold_in(folded_values, 3), (3,), 0, SEQUENCE_TOKENS)
    loss_values = jnp.log(jax.random.uniform(jax.random.fold_in(folded_values, 4), (3, GROUPS), jnp.float32, 0.65, 0.8))
    spike_mask = (jnp.arange(SEQUENCE_TOKENS)[None, :] == spike_locations[:, None]).astype(jnp.float32)
    return steady_state + jnp.einsum('aw,ay->wy', loss_values, spike_mask)


def steps_of(rng, dims, pieces, low, largest):
    loudness, own = 1.0, jax.random.fold_in(rng, 6)
    for dim, parts in pieces:
        heights = jnp.exp(jax.random.uniform(jax.random.fold_in(own, dim), (parts,), jnp.float32, low / len(pieces), largest / len(pieces)))
        loudness = loudness * jnp.repeat(heights, dims[dim] // parts).reshape([-1 if axis == dim else 1 for axis in range(len(dims))])
    return loudness


def shared_out(rng, own, number, rows, amount, top, most, skew):
    sequence = jax.random.permutation(rng, amount)
    heavy_load, usual = portions_of(amount, rows * top, most, skew, True), portions_of(amount, rows * top, most, skew, False)
    places = jnp.arange(amount)

    def named(tallies, turn):
        used = int((tallies > 0).sum())
        fixed = max(1, used // 4)
        moved = fixed + (places - fixed + turn * (used - fixed)) % max(1, amount - fixed)
        return jnp.zeros((amount,), jnp.int32).at[sequence[jnp.where(places < fixed, places, moved)]].set(jnp.asarray(tallies, jnp.int32))

    tallies = jnp.where(number % 4 == 0, named(heavy_load, number // 4), named(usual, number - number // 4 - 1))
    mixed = jax.random.permutation(jax.random.fold_in(own, 3), amount)
    source_of, receiver = mixed[0:amount // 2 * 2:2], mixed[1:amount // 2 * 2:2]
    margin = jnp.minimum(tallies[source_of] - 1, most - tallies[receiver]) // 2
    margin = jnp.where((source_of == sequence[0]) | (receiver == sequence[0]) | (tallies[receiver] == 0), 0, jnp.maximum(margin, 0))
    moved = jax.random.randint(jax.random.fold_in(own, 4), (amount // 2,), 0, 1 << 20) % (margin + 1)
    tallies = tallies.at[source_of].add(-moved).at[receiver].add(moved)
    labels = jnp.searchsorted(jnp.cumsum(tallies), jnp.arange(rows * top), side="right").astype(jnp.int32)
    listing = labels.reshape(top, rows).T
    listing = listing[jax.random.permutation(jax.random.fold_in(own, 1), rows)]
    turn = jax.random.randint(jax.random.fold_in(own, 2), (rows, 1), 0, top)
    return jnp.take_along_axis(listing, (jnp.arange(top)[None, :] + turn) % top, axis=1)


def portions_of(amount, total, most, slope, full):
    loads = [(1 << 20) // math.isqrt(rank ** slope) + 1 for rank in range(1, amount + 1)]
    largest = most if full else min(most, max(-(-total // amount), total * loads[0] // sum(loads)))
    least = 1 if total - largest >= amount - 1 else 0
    given, surplus = [largest] + [least] * (amount - 1), total - largest - least * (amount - 1)
    while surplus > 0:
        candidates = [i for i in range(1, amount) if given[i] < largest] or [i for i in range(1, amount) if given[i] < most]
        mass, budget = sum([loads[i] for i in candidates]), surplus
        for i in candidates:
            more = min(most - given[i], max(1, budget * loads[i] // mass), surplus)
            given[i] = given[i] + more
            surplus = surplus - more
    return np.array(given)


def noise(own_key, shape, width, reach, split=(), kind=jnp.bfloat16):
    gain = steps_of(own_key, shape, split, -0.22, 0.18) if split else 1.0
    drawn = jax.random.normal(own_key, shape, jnp.float32) * width * gain
    return jnp.minimum(jnp.maximum(drawn, -reach), reach).astype(kind)


def setup_inputs(seed: int = 0) -> dict:
    seeds = jax.random.split(jax.random.key(seed), 21)
    mixer_input = noise(seeds[0], (SEQUENCE_TOKENS, MIX_WIDTH), 1.0, 6.0, ((0, 8), (1, 4)))
    retention = draw_retention(jax.random.fold_in(seeds[20], 71), 0)
    decay_real = draw_decay_real(jax.random.fold_in(seeds[20], 71), 0)
    decay_freq = draw_decay_freq(jax.random.fold_in(seeds[20], 71), 0)
    log_step = draw_log_step(jax.random.fold_in(seeds[20], 71), 0)
    input_real = draw_input_real(jax.random.fold_in(seeds[20], 71), 0)
    input_imag = draw_input_imag(jax.random.fold_in(seeds[20], 71), 0)
    readout_real = noise(seeds[7], (GROUPS, CHANNELS, STATE), (2 * STATE) ** -0.5, 0.5, ((0, 4),), jnp.float32)
    readout_imaginary = noise(seeds[8], (GROUPS, CHANNELS, STATE), (2 * STATE) ** -0.5, 0.5, ((0, 4),), jnp.float32)
    skip_weight = noise(seeds[9], (GROUPS, CHANNELS), 1.0, 4.0, ((0, 4),), jnp.float32)
    norm_gain = jnp.clip(1.0 + 0.18 * jax.random.normal(seeds[10], (MIX_WIDTH,), jnp.float32), 0.1, 1.9)
    projection = noise(seeds[11], (MIX_WIDTH, WIDTH), MIX_WIDTH ** -0.5, 0.1875, ((0, 4),))
    residual = noise(seeds[12], (SEQUENCE_TOKENS, WIDTH), 1.0, 6.0, ((0, 32),))
    mix_gain = jnp.clip(1.0 + 0.18 * jax.random.normal(seeds[13], (WIDTH,), jnp.float32), 0.1, 1.9)
    routes_keys = jax.random.split(jax.random.fold_in(seeds[14], 1), SEQUENCE_TOKENS // DEVICE_ROWS)
    routes_turns = jax.random.permutation(jax.random.fold_in(seeds[14], 3), SEQUENCE_TOKENS // DEVICE_ROWS)
    routes = jax.vmap(lambda own, number: shared_out(jax.random.fold_in(seeds[14], 2), own, number, DEVICE_ROWS, EXPERTS, PICKS, CAPACITY, 2))(routes_keys, routes_turns).reshape((SEQUENCE_TOKENS, PICKS))
    route_weight = jnp.clip(0.5 + 1.5 * jax.random.uniform(seeds[15], (SEQUENCE_TOKENS, PICKS), jnp.float32) ** steps_of(seeds[15], (SEQUENCE_TOKENS, PICKS), ((0, 32),), -0.2, 0.2), 0.5, 2.0)
    expert_gate = noise(seeds[16], (EXPERTS, WIDTH, EXPERT_HIDDEN), WIDTH ** -0.5, 0.125, ((0, 8),))
    expert_up = noise(seeds[17], (EXPERTS, WIDTH, EXPERT_HIDDEN), WIDTH ** -0.5, 0.125, ((0, 8),))
    expert_down = noise(seeds[18], (EXPERTS, EXPERT_HIDDEN, WIDTH), EXPERT_HIDDEN ** -0.5, 0.25, ((0, 8),))
    final_gain = jnp.clip(1.0 + 0.18 * jax.random.normal(seeds[19], (WIDTH,), jnp.float32), 0.1, 1.9)
    return dict(mixer_input=mixer_input, retention=retention, decay_real=decay_real, decay_freq=decay_freq, log_step=log_step, input_real=input_real, input_imag=input_imag, readout_real=readout_real, readout_imaginary=readout_imaginary, skip_weight=skip_weight, norm_gain=norm_gain, projection=projection, residual=residual, mix_gain=mix_gain, routes=routes, route_weight=route_weight, expert_gate=expert_gate, expert_up=expert_up, expert_down=expert_down, final_gain=final_gain)


deep_alpha = 2.0 ** 0.25
highest_precision = lax.Precision.HIGHEST
row_block = 512

def input_factor(decay_real, decay_freq, log_step):
    stride = jnp.exp(log_step)[:, None]
    growth = decay_real * stride
    turning = decay_freq * stride
    upper_real = jnp.expm1(growth) * jnp.cos(turning) - 2.0 * jnp.sin(0.5 * turning) ** 2
    upper_imag = jnp.exp(growth) * jnp.sin(turning)
    denominator = decay_real * decay_real + decay_freq * decay_freq
    factor_real = (upper_real * decay_real + upper_imag * decay_freq) / denominator
    factor_imag = (upper_imag * decay_real - upper_real * decay_freq) / denominator
    return (growth, turning, factor_real, factor_imag)

def layer_norm(values, scales):
    centered = values - lax.optimization_barrier(jnp.mean(values, axis=-1, keepdims=True))
    variance = lax.optimization_barrier(jnp.mean(centered * centered, axis=-1, keepdims=True))
    return centered * lax.rsqrt(variance + 1e-05) * scales

def reference(mixer_input, retention, decay_real, decay_freq, log_step, input_real, input_imag, readout_real, readout_imaginary, skip_weight, norm_gain, projection, residual, mix_gain, routes, route_weight, expert_gate, expert_up, expert_down, final_gain):
    growth, turning, factor_real, factor_imag = input_factor(decay_real, decay_freq, log_step)
    keep_real = jnp.exp(growth) * jnp.cos(turning)
    keep_imag = jnp.exp(growth) * jnp.sin(turning)
    bar_real = factor_real[:, :, None] * input_real - factor_imag[:, :, None] * input_imag
    bar_imag = factor_real[:, :, None] * input_imag + factor_imag[:, :, None] * input_real
    inputs = mixer_input.reshape(SEQUENCE_TOKENS, GROUPS, CHANNELS)
    held_log = jnp.transpose(retention)

    def advance(carried, position):
        state_real_part, state_imaginary = carried
        current, kept_log = position
        current = current.astype(jnp.float32)
        shrink = jnp.exp(kept_log)[:, None]
        drive_real = jnp.einsum('gpc,gc->gp', bar_real, current, precision=highest_precision)
        drive_imag = jnp.einsum('gpc,gc->gp', bar_imag, current, precision=highest_precision)
        following_real = shrink * (keep_real * state_real_part - keep_imag * state_imaginary) + drive_real
        following_imaginary = shrink * (keep_real * state_imaginary + keep_imag * state_real_part) + drive_imag
        readout_result = jnp.einsum('zhy,zy->zh', readout_real, following_real, precision=highest_precision)
        readout_result = readout_result - jnp.einsum('zhy,zy->zh', readout_imaginary, following_imaginary, precision=highest_precision)
        readout_result = readout_result + skip_weight * current
        return ((following_real, following_imaginary), jax.nn.gelu(readout_result).astype(jnp.bfloat16))
    zero_state = jnp.zeros((GROUPS, STATE), jnp.float32)
    ignored_state, mixed_seq = lax.scan(advance, (zero_state, zero_state), (inputs, held_log))
    mixed_seq = mixed_seq.reshape(SEQUENCE_TOKENS, MIX_WIDTH)
    mixed_float = mixed_seq.astype(jnp.float32)
    row_square = lax.optimization_barrier(jnp.mean(mixed_float * mixed_float, axis=1))
    scaled = (mixed_float * norm_gain).astype(jnp.bfloat16)
    mix = jnp.dot(scaled, projection, preferred_element_type=jnp.float32) * lax.rsqrt(row_square + 1e-06)[:, None]
    hidden = layer_norm(deep_alpha * residual.astype(jnp.float32) + mix, mix_gain).astype(jnp.bfloat16)
    hidden_pad = jnp.concatenate([hidden, jnp.zeros((1, WIDTH), hidden.dtype)], axis=0)
    assigned = routes.reshape(-1).astype(jnp.int32)
    sort_order = jnp.argsort(assigned, stable=True).astype(jnp.int32)
    sorted_expert = assigned[sort_order]
    sorted_token = (sort_order // PICKS).astype(jnp.int32)
    sorted_weight = route_weight.reshape(-1)[sort_order]
    expert_load = lax.optimization_barrier(jnp.sum((assigned[:, None] == jnp.arange(EXPERTS, dtype=jnp.int32)[None, :]).astype(jnp.int32), axis=0))
    padded_rows = (expert_load + row_block - 1) // row_block * row_block
    padded_end = jnp.cumsum(padded_rows).astype(jnp.int32)
    padded_start = padded_end - padded_rows
    first_sorted = (jnp.cumsum(expert_load) - expert_load).astype(jnp.int32)
    assigned_count = SEQUENCE_TOKENS * PICKS
    dest_slot = padded_start[sorted_expert] + jnp.arange(assigned_count, dtype=jnp.int32) - first_sorted[sorted_expert]
    block_total = (assigned_count + EXPERTS * row_block) // row_block + 1
    buffer_rows = block_total * row_block
    token_buffer = jnp.full((buffer_rows,), SEQUENCE_TOKENS, jnp.int32).at[dest_slot].set(sorted_token)
    weight_buffer = jnp.zeros((buffer_rows,), route_weight.dtype).at[dest_slot].set(sorted_weight)
    block_starts = jnp.arange(block_total, dtype=jnp.int32) * row_block
    block_expert = lax.optimization_barrier(jnp.sum((padded_end[None, :] <= block_starts[:, None]).astype(jnp.int32), axis=1))
    block_expert = jnp.minimum(block_expert, EXPERTS - 1).astype(jnp.int32)

    def one_block(running, block_items):
        tokens_here, weights_here, expert_here = block_items
        rows_here = hidden_pad[tokens_here]
        gate_act = jnp.dot(rows_here, expert_gate[expert_here], preferred_element_type=jnp.float32)
        up_act = jnp.dot(rows_here, expert_up[expert_here], preferred_element_type=jnp.float32)
        active = (jax.nn.silu(gate_act) * up_act).astype(jnp.bfloat16)
        produced = jnp.dot(active, expert_down[expert_here], preferred_element_type=jnp.float32).astype(jnp.bfloat16)
        return (running.at[tokens_here].add(weights_here[:, None] * produced.astype(jnp.float32)), None)
    mix_init = jnp.zeros((SEQUENCE_TOKENS + 1, WIDTH), jnp.float32)
    expert_mix, ignored = lax.scan(one_block, mix_init, (token_buffer.reshape(block_total, row_block), weight_buffer.reshape(block_total, row_block), block_expert))
    layer_out = layer_norm(deep_alpha * hidden.astype(jnp.float32) + expert_mix[:SEQUENCE_TOKENS], final_gain)
    return layer_out.astype(jnp.bfloat16)
```

```python
import functools

import jax
import jax.numpy as jnp
from jax import lax
from jax.experimental import pallas as pl
from jax.experimental.pallas import tpu as pltpu
from jax.sharding import PartitionSpec as P

PICKS = 2
SPANS = 8
deep_alpha = 2.0**0.25
f32, bf16 = jnp.float32, jnp.bfloat16
highest = lax.Precision.HIGHEST
NT = (((1,), (1,)), ((), ()))
TN = (((0,), (0,)), ((), ()))
PROJ_CHUNKS = 4


def dot(a, b, dims=None, precision=None):
    dims = dims or (((1,), (0,)), ((), ()))
    return lax.dot_general(a, b, dims, precision=precision, preferred_element_type=f32)


def split(value):
    high = value.astype(bf16)
    return high, (value - high.astype(f32)).astype(bf16)


def iota(shape, dim):
    return lax.broadcasted_iota(jnp.int32, shape, dim)


def layer_norm(values, scales):
    centered = values - jnp.mean(values, axis=-1, keepdims=True)
    variance = jnp.mean(centered * centered, axis=-1, keepdims=True)
    return centered * lax.rsqrt(variance + 1e-05) * scales


def cmul(ar, ai, br, bi):
    return ar * br - ai * bi, ar * bi + ai * br


def expm1(value, grown):
    series = value * 0.125 + 1.0
    for k in range(7, 1, -1):
        series = series * value * (1.0 / k) + 1.0
    return jnp.where(value > -0.4, series * value, grown - 1.0)


def repeat(count, body):
    if count <= 8:
        for k in range(count):
            body(k)
    else:
        lax.fori_loop(0, count, lambda k, c: (body(k), c)[1], 0)


def kernel(
    n_sp, n_tp, groups, channels, states, cap,
    x_hbm, ret_hbm, real_hbm, freq_hbm, step_hbm, skip_hbm, gain_hbm, in_re_hbm, in_im_hbm,
    out_re_hbm, out_im_hbm, res_hbm, mix_gain_hbm, routes_hbm, rw_hbm, final_gain_hbm,
    proj_ref, gate_ref, up_ref, down_ref,
    o_ref,
    x_ref, ret_ref, real_ref, freq_ref, step_ref, skip_ref, gain_ref, in_re_ref, in_im_ref,
    out_re_ref, out_im_ref, res_ref, mix_gain_ref, routes_ref, rw_ref, final_gain_ref,
    d_re, d_im, shr, carry_out, carry_in, mix_out, mix_in, proj_all, gate_v, up_v, down_v,
    acc, hid, tok_out, tok_in, ret_out, ret_in,
    in_sem, w_sem, car_s, car_r, mix_s, mix_r, prj_s, prj_r, fwd_s, fwd_r, tok_s, tok_r, back_s, back_r,
):
    sp, tp = lax.axis_index("sp"), lax.axis_index("tp")
    tokens, chans = x_ref.shape
    gp = groups * states
    span = tokens // SPANS
    rows = tokens // n_tp
    width = o_ref.shape[1]

    small = (
        (step_hbm, step_ref), (real_hbm, real_ref), (freq_hbm, freq_ref), (in_re_hbm, in_re_ref),
        (in_im_hbm, in_im_ref), (x_hbm, x_ref), (ret_hbm, ret_ref), (skip_hbm, skip_ref),
        (out_re_hbm, out_re_ref), (out_im_hbm, out_im_ref), (gain_hbm, gain_ref),
        (routes_hbm, routes_ref), (rw_hbm, rw_ref), (res_hbm, res_ref),
        (mix_gain_hbm, mix_gain_ref), (final_gain_hbm, final_gain_ref),
    )
    fetches = [
        pltpu.make_async_copy(src, dst, in_sem.at[i]) for i, (src, dst) in enumerate(small)
    ]
    for fetch in fetches:
        fetch.start()

    barrier = pltpu.get_barrier_semaphore()

    def greet_sp(k):
        pl.semaphore_signal(barrier, inc=1, device_id={"sp": lax.rem(sp + k + 1, n_sp)})

    def greet_tp(k):
        pl.semaphore_signal(barrier, inc=1, device_id={"tp": lax.rem(tp + k + 1, n_tp)})

    repeat(n_sp - 1, greet_sp)
    repeat(n_tp - 1, greet_tp)

    own = pltpu.make_async_copy(proj_ref, proj_all.at[tp], w_sem.at[0])
    own.start()
    loads = [own]
    for i, (src, dst) in enumerate(((gate_ref, gate_v), (up_ref, up_v), (down_ref, down_v))):
        loads.append(pltpu.make_async_copy(src.at[0], dst, w_sem.at[i + 1]))
        loads[-1].start()
    pl.semaphore_wait(barrier, n_sp - 1 + n_tp - 1)

    depth = proj_ref.shape[0] // PROJ_CHUNKS
    near = tp + 1 - 2 * lax.rem(tp, 2)
    far = lax.rem(tp + 2, n_tp)

    def piece(i):
        return pl.ds(i * depth, depth)

    proj_far = [
        pltpu.make_async_remote_copy(
            proj_ref.at[piece(i)], proj_all.at[tp, piece(i)], prj_s.at[i], prj_r.at[i],
            device_id={"tp": far},
        )
        for i in range(PROJ_CHUNKS)
    ]
    proj_near = pltpu.make_async_remote_copy(
        proj_ref, proj_all.at[tp], prj_s.at[PROJ_CHUNKS], prj_r.at[PROJ_CHUNKS],
        device_id={"tp": near},
    )
    proj_fwd = [
        pltpu.make_async_remote_copy(
            proj_all.at[far, piece(i)], proj_all.at[far, piece(i)], fwd_s.at[i], fwd_r.at[i],
            device_id={"tp": near},
        )
        for i in range(PROJ_CHUNKS)
    ]
    for copy in proj_far:
        copy.start()
    proj_near.start()

    for fetch in fetches:
        fetch.wait()

    eye = iota((groups, groups), 0) == iota((groups, groups), 1)
    stride = jnp.exp(jnp.sum(jnp.where(eye, step_ref[...], 0.0), axis=1, keepdims=True))
    real, freq = real_ref[...], freq_ref[...]
    growth, turning = real * stride, freq * stride
    cosine, sine, half = jnp.cos(turning), jnp.sin(turning), jnp.sin(0.5 * turning)
    size = jnp.exp(growth)
    upper_real = expm1(growth, size) * cosine - 2.0 * half * half
    keep_re, upper_imag = size * cosine, size * sine
    denominator = real * real + freq * freq
    f_re = (upper_real * real + upper_imag * freq) / denominator
    f_im = (upper_imag * real - upper_real * freq) / denominator
    big_re, big_im = keep_re, upper_imag
    for _ in range(span.bit_length() - 1):
        big_re, big_im = cmul(big_re, big_im, big_re, big_im)

    tile_p = jnp.where(
        lax.rem(iota((states, gp), 1), states) == iota((states, gp), 0), 1.0, 0.0
    )
    widen = jnp.where(
        iota((groups, gp), 1) // states == iota((groups, gp), 0), 1.0, 0.0
    ).astype(f32)
    packed = jnp.concatenate([keep_re, upper_imag, big_re, big_im], axis=0)
    spread = dot(packed, tile_p, precision=highest)
    k_re, k_im, b_re, b_im = [
        jnp.sum(spread[i * groups : (i + 1) * groups] * widen, axis=0, keepdims=True)
        for i in range(4)
    ]
    tile_p = tile_p.astype(bf16)
    mask_out = iota((chans, gp), 0) // channels == iota((chans, gp), 1) // states

    def wide(value):
        return [
            jnp.where(mask_out, dot(part, tile_p), 0.0).astype(bf16) for part in split(value)
        ]

    copies = jnp.where(
        iota((chans, groups), 0) // channels == iota((chans, groups), 1), 1.0, 0.0
    ).astype(f32)
    f_re, f_im = dot(copies, f_re, precision=highest), dot(copies, f_im, precision=highest)
    bar_re, bar_im = cmul(f_re, f_im, in_re_ref[...], in_im_ref[...])

    row_i, col_i = iota((tokens, tokens), 0), iota((tokens, tokens), 1)
    perm = jnp.where(
        col_i == lax.rem(row_i, SPANS) * span + row_i // SPANS, 1.0, 0.0
    ).astype(bf16)
    x = dot(perm, x_ref[...]).astype(bf16)
    for bar, d_ref in ((bar_re, d_re), (bar_im, d_im)):
        high, low = wide(bar)
        d_ref[...] = dot(x, high) + dot(x, low)
    held = dot(jnp.exp(ret_ref[...]), perm.astype(f32), NT, precision=highest)
    shr[...] = dot(held, widen, TN, precision=highest)

    k_re = jnp.broadcast_to(k_re, (SPANS, gp))
    k_im = jnp.broadcast_to(k_im, (SPANS, gp))

    def advance(j, s_re, s_im):
        at = pl.ds(pl.multiple_of(j * SPANS, SPANS), SPANS)
        m_re, m_im = cmul(k_re, k_im, s_re, s_im)
        shrink = shr[at, :]
        return at, shrink, shrink * m_re + d_re[at, :], shrink * m_im + d_im[at, :]

    def first(j, state):
        s_re, s_im, total = state
        _, shrink, s_re, s_im = advance(j, s_re, s_im)
        return s_re, s_im, total * shrink

    zero = jnp.zeros((SPANS, gp), f32)
    e_re, e_im, total = lax.fori_loop(0, span, first, (zero, zero, zero + 1.0))
    a_re, a_im = total * b_re, total * b_im

    one = jnp.ones((1, gp), f32)
    nil = jnp.zeros((1, gp), f32)
    c_re, c_im, s_re, s_im = one, nil, nil, nil
    entries = []
    for i in range(SPANS):
        entries.append((c_re, c_im, s_re, s_im))
        ar, ai = a_re[i : i + 1], a_im[i : i + 1]
        s_re, s_im = cmul(ar, ai, s_re, s_im)
        s_re, s_im = s_re + e_re[i : i + 1], s_im + e_im[i : i + 1]
        c_re, c_im = cmul(ar, ai, c_re, c_im)
    for i, part in enumerate((c_re, c_im, s_re, s_im)):
        carry_out[i : i + 1, :] = part

    def carry_copy(k):
        return pltpu.make_async_remote_copy(
            carry_out, carry_in.at[sp], car_s.at[k], car_r.at[k],
            device_id={"sp": lax.rem(sp + k + 1, n_sp)},
        )

    repeat(n_sp - 1, lambda k: carry_copy(k).start())
    c_re, c_im, s_re, s_im = [
        jnp.concatenate([entry[i] for entry in entries], axis=0) for i in range(4)
    ]

    o_re, o_im = wide(out_re_ref[...]), wide(out_im_ref[...])
    tile_c = jnp.where(
        lax.rem(iota((channels, chans), 1), channels) == iota((channels, chans), 0), 1.0, 0.0
    ).astype(f32)
    own_group = iota((groups, chans), 1) // channels == iota((groups, chans), 0)
    skip = jnp.where(own_group, dot(skip_ref[...], tile_c, precision=highest), 0.0)
    skip = jnp.sum(skip, axis=0, keepdims=True)

    repeat(n_sp - 1, lambda k: carry_copy(k).wait_recv())

    def fold(position, state):
        part = carry_in[position]
        n_re, n_im = cmul(part[0:1], part[1:2], *state)
        return (
            jnp.where(position < sp, n_re + part[2:3], state[0]),
            jnp.where(position < sp, n_im + part[3:4], state[1]),
        )

    state = (nil, nil)
    if n_sp <= 8:
        for position in range(n_sp - 1):
            state = fold(position, state)
    else:
        state = lax.fori_loop(0, n_sp - 1, fold, state)
    m_re, m_im = cmul(c_re, c_im, *state)

    def second(j, state):
        at, _, s_re, s_im = advance(j, *state)
        d_re[at, :] = s_re
        d_im[at, :] = s_im
        return s_re, s_im

    lax.fori_loop(0, span, second, (s_re + m_re, s_im + m_im))

    def read(ref, wide):
        high, low = split(ref[...])
        return dot(high, wide[0], NT) + dot(low, wide[0], NT) + dot(high, wide[1], NT)

    y = read(d_re, o_re) - read(d_im, o_im) + skip * x.astype(f32)
    y = jax.nn.gelu(y).astype(bf16)
    mix_out[...] = dot(perm, y, TN).astype(bf16)

    def mine(index):
        return pl.ds(pl.multiple_of(index * rows, rows), rows)

    mixes = []
    for k in range(n_tp - 1):
        peer = lax.rem(tp + k + 1, n_tp)
        mixes.append(
            pltpu.make_async_remote_copy(
                mix_out.at[mine(peer)], mix_in.at[tp], mix_s.at[k], mix_r.at[k],
                device_id={"tp": peer},
            )
        )
        mixes[-1].start()
    mix_in[tp] = mix_out[mine(tp), :]

    slots = n_sp * cap
    expert_of = iota((slots, rows), 0) // cap
    hit0 = routes_ref[0:1, :] == expert_of
    hit1 = routes_ref[1:2, :] == expert_of
    member = jnp.where(hit0 | hit1, 1.0, 0.0)
    upper = jnp.where(iota((rows, rows), 0) < iota((rows, rows), 1), 1.0, 0.0).astype(bf16)
    place = dot(member.astype(bf16), upper)
    wanted = lax.rem(iota((slots, rows), 0), cap).astype(f32)
    chosen = jnp.where(place == wanted, member, 0.0)
    weight = chosen * jnp.where(hit0, rw_ref[0:1, :], rw_ref[1:2, :])
    chosen = chosen.astype(bf16)

    for i in range(PROJ_CHUNKS):
        proj_far[i].wait_recv()
        proj_fwd[i].start()
    for copy in mixes:
        copy.wait_recv()
    own.wait()
    proj_near.wait_recv()
    squares = jnp.zeros((rows, 1), f32)
    scaled = []
    for s in range(n_tp):
        part = mix_in[s].astype(f32)
        squares += jnp.sum(part * part, axis=1, keepdims=True)
        scaled.append((part * gain_ref[:, s * chans : (s + 1) * chans]).astype(bf16))
    scale = lax.rsqrt(squares / (n_tp * chans) + 1e-06)
    for copy in proj_fwd:
        copy.wait_recv()
    wide = 256

    def project(i, c):
        cols = pl.ds(pl.multiple_of(i * wide, wide), wide)
        part = dot(scaled[0], proj_all[0, :, cols])
        for s in range(1, n_tp):
            part += dot(scaled[s], proj_all[s, :, cols])
        acc[:, cols] = deep_alpha * res_ref[:, cols].astype(f32) + part * scale
        return c

    lax.fori_loop(0, width // wide, project, 0)
    hid[...] = layer_norm(acc[...], mix_gain_ref[...]).astype(bf16)

    def route_out(i, c):
        cols = pl.ds(pl.multiple_of(i * wide, wide), wide)
        tok_out[:, :, cols] = dot(chosen, hid[:, cols]).astype(bf16).reshape(n_sp, cap, wide)
        return c

    lax.fori_loop(0, width // wide, route_out, 0)

    def tok_copy(k):
        peer = lax.rem(sp + k + 1, n_sp)
        return pltpu.make_async_remote_copy(
            tok_out.at[peer], tok_in.at[sp], tok_s.at[k], tok_r.at[k], device_id={"sp": peer}
        )

    repeat(n_sp - 1, lambda k: tok_copy(k).start())
    tok_in[sp] = tok_out[sp]
    for copy in loads[1:]:
        copy.wait()
    repeat(n_sp - 1, lambda k: tok_copy(k).wait_recv())

    arrived = tok_in[...].reshape(slots, width)
    gate = dot(arrived, gate_v[...])
    up = dot(arrived, up_v[...])
    active = (gate * jax.nn.sigmoid(gate) * up).astype(bf16)

    def produce(i, c):
        cols = pl.ds(pl.multiple_of(i * wide, wide), wide)
        ret_out[:, :, cols] = dot(active, down_v[:, cols]).astype(bf16).reshape(n_sp, cap, wide)
        return c

    lax.fori_loop(0, width // wide, produce, 0)

    def back_copy(k):
        peer = lax.rem(sp + k + 1, n_sp)
        return pltpu.make_async_remote_copy(
            ret_out.at[peer], ret_in.at[sp], back_s.at[k], back_r.at[k], device_id={"sp": peer}
        )

    repeat(n_sp - 1, lambda k: back_copy(k).start())
    ret_in[sp] = ret_out[sp]
    w_high, w_low = split(weight)
    repeat(n_sp - 1, lambda k: back_copy(k).wait_recv())

    def combine(i, c):
        cols = pl.ds(pl.multiple_of(i * wide, wide), wide)
        got = ret_in[:, :, cols].reshape(slots, wide)
        acc[:, cols] = (
            deep_alpha * hid[:, cols].astype(f32) + dot(w_high, got, TN) + dot(w_low, got, TN)
        )
        return c

    lax.fori_loop(0, width // wide, combine, 0)
    o_ref[...] = layer_norm(acc[...], final_gain_ref[...]).astype(bf16)

    for copy in proj_far + [proj_near] + proj_fwd + mixes:
        copy.wait_send()
    repeat(n_sp - 1, lambda k: carry_copy(k).wait_send())
    repeat(n_sp - 1, lambda k: tok_copy(k).wait_send())
    repeat(n_sp - 1, lambda k: back_copy(k).wait_send())


def local(
    mixer_input, retention, decay_real, decay_freq, log_step, input_real, input_imag,
    readout_real, readout_imaginary, skip_weight, norm_gain, projection, residual, mix_gain,
    routes, route_weight, expert_gate, expert_up, expert_down, final_gain,
):
    n_sp, n_tp = lax.axis_size("sp"), lax.axis_size("tp")
    tokens, chans = mixer_input.shape
    groups, states, channels = input_real.shape
    gp, rows, width = groups * states, residual.shape[0], residual.shape[1]
    cap = -(-max(2, 2 * rows * PICKS // n_sp) // 16) * 16
    hidden = expert_gate.shape[2]

    def compact(value):
        return jnp.swapaxes(value, 1, 2).reshape(chans, states)

    small = (
        mixer_input, retention, decay_real, decay_freq, log_step[None, :], skip_weight,
        norm_gain[None, :], compact(input_real), compact(input_imag),
        readout_real.reshape(chans, states), readout_imaginary.reshape(chans, states),
        residual, mix_gain[None, :], routes.T, route_weight.T, final_gain[None, :],
    )
    vmem = pl.BlockSpec(memory_space=pltpu.VMEM)
    anywhere = pl.BlockSpec(memory_space=pl.ANY)
    dma = pltpu.SemaphoreType.DMA
    return pl.pallas_call(
        functools.partial(kernel, n_sp, n_tp, groups, channels, states, cap),
        out_shape=jax.ShapeDtypeStruct((rows, width), bf16),
        in_specs=[anywhere] * (len(small) + 4),
        out_specs=vmem,
        scratch_shapes=[pltpu.VMEM(value.shape, value.dtype) for value in small]
        + [
            pltpu.VMEM((tokens, gp), f32),
            pltpu.VMEM((tokens, gp), f32),
            pltpu.VMEM((tokens, gp), f32),
            pltpu.VMEM((4, gp), f32),
            pltpu.VMEM((n_sp, 4, gp), f32),
            pltpu.VMEM((tokens, chans), bf16),
            pltpu.VMEM((n_tp, rows, chans), bf16),
            pltpu.VMEM((n_tp,) + projection.shape, bf16),
            pltpu.VMEM((width, hidden), bf16),
            pltpu.VMEM((width, hidden), bf16),
            pltpu.VMEM((hidden, width), bf16),
            pltpu.VMEM((rows, width), f32),
            pltpu.VMEM((rows, width), bf16),
            pltpu.VMEM((n_sp, cap, width), bf16),
            pltpu.VMEM((n_sp, cap, width), bf16),
            pltpu.VMEM((n_sp, cap, width), bf16),
            pltpu.VMEM((n_sp, cap, width), bf16),
            dma((len(small),)), dma((4,)),
            dma((n_sp,)), dma((n_sp,)),
            dma((n_tp,)), dma((n_tp,)),
            dma((PROJ_CHUNKS + 1,)), dma((PROJ_CHUNKS + 1,)),
            dma((PROJ_CHUNKS,)), dma((PROJ_CHUNKS,)),
            dma((n_sp,)), dma((n_sp,)),
            dma((n_sp,)), dma((n_sp,)),
        ],
        compiler_params=pltpu.CompilerParams(
            collective_id=0, has_side_effects=True, vmem_limit_bytes=60 * 1024 * 1024
        ),
    )(
        *small,
        projection, expert_gate, expert_up, expert_down,
    )


def solution(mesh):
    in_specs = (
        P("sp", "tp"),
        P("tp", "sp"),
        P("tp", None),
        P("tp", None),
        P("tp"),
        P("tp", None, None),
        P("tp", None, None),
        P("tp", None, None),
        P("tp", None, None),
        P("tp", None),
        P(),
        P("tp", None),
        P(("sp", "tp"), None),
        P(),
        P(("sp", "tp"), None),
        P(("sp", "tp"), None),
        P("sp", None, None),
        P("sp", None, None),
        P("sp", None, None),
        P(),
    )
    out_specs = P(("sp", "tp"), None)
    return jax.shard_map(local, mesh=mesh, in_specs=in_specs, out_specs=out_specs, check_vma=False)
```

```python
import functools

import jax
import jax.numpy as jnp
from jax import lax
from jax.experimental import pallas as pl
from jax.experimental.pallas import tpu as pltpu
from jax.sharding import PartitionSpec as P

PICKS = 2
SPANS = 8
deep_alpha = 2.0**0.25
f32, bf16 = jnp.float32, jnp.bfloat16
highest = lax.Precision.HIGHEST
NT = (((1,), (1,)), ((), ()))
TN = (((0,), (0,)), ((), ()))
PROJ_CHUNKS = 8
PROJ_FIRST = 3
LO = 2
HALVES = 2
BATCH_ROWS = 128


def dot(a, b, dims=None, precision=None):
    dims = dims or (((1,), (0,)), ((), ()))
    return lax.dot_general(a, b, dims, precision=precision, preferred_element_type=f32)


def split(value):
    high = value.astype(bf16)
    return high, (value - high.astype(f32)).astype(bf16)


def iota(shape, dim):
    return lax.broadcasted_iota(jnp.int32, shape, dim)


def layer_norm(values, scales):
    centered = values - jnp.mean(values, axis=-1, keepdims=True)
    variance = jnp.mean(centered * centered, axis=-1, keepdims=True)
    return centered * lax.rsqrt(variance + 1e-05) * scales


def cmul(ar, ai, br, bi):
    return ar * br - ai * bi, ar * bi + ai * br


def expm1(value, grown):
    series = value * 0.125 + 1.0
    for k in range(7, 1, -1):
        series = series * value * (1.0 / k) + 1.0
    return jnp.where(value > -0.4, series * value, grown - 1.0)


def repeat(count, body):
    if count <= 8:
        for k in range(count):
            body(k)
    else:
        lax.fori_loop(0, count, lambda k, c: (body(k), c)[1], 0)


def kernel(
    n_sp, n_tp, groups, channels, states, cap,
    x_hbm, ret_hbm, real_hbm, freq_hbm, step_hbm, skip_hbm, gain_hbm, in_re_hbm, in_im_hbm,
    out_re_hbm, out_im_hbm, res_hbm, mix_gain_hbm, routes_hbm, rw_hbm, final_gain_hbm,
    proj_ref, gate_ref, up_ref, down_ref,
    o_ref,
    x_ref, ret_ref, real_ref, freq_ref, step_ref, skip_ref, gain_ref, in_re_ref, in_im_ref,
    out_re_ref, out_im_ref, res_ref, mix_gain_ref, routes_ref, rw_ref, final_gain_ref,
    d_re, d_im, shr, carry_out, carry_in, mix_out, mix_in, proj_all, gate_v, up_v, down_v,
    acc, hid, scaled_v, acc_b, hid_b, pick_out, pick_in, raw, res_out, res_in, y_out, y_in,
    ret_out, ret_in,
    in_sem, w_sem, car_s, car_r, mix_s, mix_r, prj_s, prj_r, fwd_s, fwd_r,
    pick_s, pick_r, up_s, up_r, low_s, low_r, res_s, res_r, y_s, y_r, back_s, back_r,
):
    sp, tp = lax.axis_index("sp"), lax.axis_index("tp")
    tokens, chans = x_ref.shape
    gp = groups * states
    span = tokens // SPANS
    rows = tokens // n_tp
    width = o_ref.shape[1]

    small = (
        (step_hbm, step_ref), (real_hbm, real_ref), (freq_hbm, freq_ref), (in_re_hbm, in_re_ref),
        (in_im_hbm, in_im_ref), (x_hbm, x_ref), (ret_hbm, ret_ref), (skip_hbm, skip_ref),
        (out_re_hbm, out_re_ref), (out_im_hbm, out_im_ref), (gain_hbm, gain_ref),
        (routes_hbm, routes_ref), (rw_hbm, rw_ref), (res_hbm, res_ref),
        (mix_gain_hbm, mix_gain_ref), (final_gain_hbm, final_gain_ref),
    )
    fetches = [
        pltpu.make_async_copy(src, dst, in_sem.at[i]) for i, (src, dst) in enumerate(small)
    ]
    for fetch in fetches:
        fetch.start()

    barrier = pltpu.get_barrier_semaphore()

    def greet_sp(k):
        pl.semaphore_signal(barrier, inc=1, device_id={"sp": lax.rem(sp + k + 1, n_sp)})

    def greet_tp(k):
        pl.semaphore_signal(barrier, inc=1, device_id={"tp": lax.rem(tp + k + 1, n_tp)})

    repeat(n_sp - 1, greet_sp)
    repeat(n_tp - 1, greet_tp)

    own = pltpu.make_async_copy(proj_ref, proj_all.at[tp], w_sem.at[0])
    own.start()
    loads = [own]
    for i, (src, dst) in enumerate(((gate_ref, gate_v), (up_ref, up_v), (down_ref, down_v))):
        loads.append(pltpu.make_async_copy(src.at[0], dst, w_sem.at[i + 1]))
        loads[-1].start()
    pl.semaphore_wait(barrier, n_sp - 1 + n_tp - 1)

    depth = proj_ref.shape[0] // PROJ_CHUNKS
    near = tp + 1 - 2 * lax.rem(tp, 2)
    far = lax.rem(tp + 2, n_tp)

    def piece(i):
        return pl.ds(i * depth, depth)

    proj_far = [
        pltpu.make_async_remote_copy(
            proj_ref.at[piece(i)], proj_all.at[tp, piece(i)], prj_s.at[i], prj_r.at[i],
            device_id={"tp": far},
        )
        for i in range(PROJ_CHUNKS)
    ]
    proj_near = pltpu.make_async_remote_copy(
        proj_ref, proj_all.at[tp], prj_s.at[PROJ_CHUNKS], prj_r.at[PROJ_CHUNKS],
        device_id={"tp": near},
    )
    proj_fwd = [
        pltpu.make_async_remote_copy(
            proj_all.at[far, piece(i)], proj_all.at[far, piece(i)], fwd_s.at[i], fwd_r.at[i],
            device_id={"tp": near},
        )
        for i in range(PROJ_CHUNKS)
    ]
    for copy in proj_far[:PROJ_FIRST]:
        copy.start()
    proj_near.start()

    for fetch in fetches:
        fetch.wait()

    slots = n_sp * cap
    expert_of = iota((slots, rows), 0) // cap
    hit0 = routes_ref[0:1, :] == expert_of
    hit1 = routes_ref[1:2, :] == expert_of
    member = jnp.where(hit0 | hit1, 1.0, 0.0)
    upper = jnp.where(iota((rows, rows), 0) < iota((rows, rows), 1), 1.0, 0.0).astype(bf16)
    place = dot(member.astype(bf16), upper)
    wanted = lax.rem(iota((slots, rows), 0), cap).astype(f32)
    chosen = jnp.where(place == wanted, member, 0.0)
    weight = chosen * jnp.where(hit0, rw_ref[0:1, :], rw_ref[1:2, :])
    chosen = chosen.astype(bf16)
    w_high, w_low = split(weight)

    def every(count, width, body):
        def step(i, c):
            body(pl.ds(pl.multiple_of(i * width, width), width))
            return c

        lax.fori_loop(0, count // width, step, 0)

    hi, lo = sp // LO, lax.rem(sp, LO)
    line = n_sp // LO
    flood = n_sp <= 8
    piece_rows = rows // HALVES

    def pick_copy(k):
        peer = lax.rem(hi + k + 1, line)
        return pltpu.make_async_remote_copy(
            pick_out.at[pl.ds(pl.multiple_of(peer * LO * cap, LO * cap), LO * cap)],
            pick_in.at[hi], pick_s.at[k], pick_r.at[k], device_id={"sp": peer * LO + lo},
        )

    def hop(sign, step, part):
        owner = lax.rem(hi - sign * step + line, line)
        piece = pl.ds(part * piece_rows, piece_rows)
        source = res_ref.at[piece] if step == 0 else raw.at[owner, piece]
        s_sem, r_sem = (up_s, up_r) if sign > 0 else (low_s, low_r)
        at = step * HALVES + part
        return pltpu.make_async_remote_copy(
            source, raw.at[owner, piece], s_sem.at[at], r_sem.at[at],
            device_id={"sp": lax.rem(sp + sign * LO + n_sp, n_sp)},
        )

    def inside(value):
        return (value >= 0) & (value < line)

    def hop_start(step, part):
        for sign in (1, -1):
            @pl.when(inside(hi - sign * step) & inside(hi + sign))
            def _():
                hop(sign, step, part).start()

    def hop_sent(step, part):
        for sign in (1, -1):
            @pl.when(inside(hi - sign * step) & inside(hi + sign))
            def _():
                hop(sign, step, part).wait_send()

    def hop_pass(step, part):
        for sign in (1, -1):
            @pl.when(inside(hi - sign * (step + 1)))
            def _():
                owner = lax.rem(hi - sign * (step + 1) + line, line)
                piece = pl.ds(part * piece_rows, piece_rows)
                s_sem, r_sem = (up_s, up_r) if sign > 0 else (low_s, low_r)
                at = step * HALVES + part
                pltpu.make_async_remote_copy(
                    raw.at[owner, piece], raw.at[owner, piece], s_sem.at[at], r_sem.at[at],
                    device_id={"sp": lax.rem(sp + LO, n_sp)},
                ).wait_recv()
        if step + 1 < line - 1:
            hop_start(step + 1, part)

    def res_copy(owner):
        return pltpu.make_async_remote_copy(
            res_out.at[owner * LO + 1 - lo], res_in.at[owner * LO + lo],
            res_s.at[owner], res_r.at[owner], device_id={"sp": hi * LO + 1 - lo},
        )

    def share(owner, pick, rows_of):
        def step(cols):
            both = dot(pick, rows_of[:, cols]).astype(bf16).reshape(LO, cap, 256)
            res_out[pl.ds(owner * LO, LO), :, cols] = both

        every(width, 256, step)
        res_in[owner * LO + lo] = res_out[owner * LO + lo]
        res_copy(owner).start()

    def share_line(step):
        for sign in (1, -1):
            @pl.when(inside(hi - sign * step))
            def _():
                owner = lax.rem(hi - sign * step + line, line)
                share(owner, pick_in[owner], raw.at[owner])

    def send_res(k):
        peer = lax.rem(sp + k + 1, n_sp)
        return pltpu.make_async_remote_copy(
            res_out.at[peer], res_in.at[sp], res_s.at[k], res_r.at[k], device_id={"sp": peer}
        )

    pick_out[...] = chosen
    if flood:
        repeat(line - 1, lambda k: pick_copy(k).start())
        hop_start(0, 0)
    else:
        def spread_res(cols):
            res_out[:, :, cols] = dot(chosen, res_ref[:, cols]).astype(bf16).reshape(n_sp, cap, 256)

        every(width, 256, spread_res)
        res_in[sp] = res_out[sp]
        repeat(n_sp - 1, lambda k: send_res(k).start())

    eye = iota((groups, groups), 0) == iota((groups, groups), 1)
    stride = jnp.exp(jnp.sum(jnp.where(eye, step_ref[...], 0.0), axis=1, keepdims=True))
    real, freq = real_ref[...], freq_ref[...]
    growth, turning = real * stride, freq * stride
    cosine, sine, half = jnp.cos(turning), jnp.sin(turning), jnp.sin(0.5 * turning)
    size = jnp.exp(growth)
    upper_real = expm1(growth, size) * cosine - 2.0 * half * half
    keep_re, upper_imag = size * cosine, size * sine
    denominator = real * real + freq * freq
    f_re = (upper_real * real + upper_imag * freq) / denominator
    f_im = (upper_imag * real - upper_real * freq) / denominator
    big_re, big_im = keep_re, upper_imag
    for _ in range(span.bit_length() - 1):
        big_re, big_im = cmul(big_re, big_im, big_re, big_im)
    full_re, full_im = big_re, big_im
    for _ in range(SPANS.bit_length() - 1):
        full_re, full_im = cmul(full_re, full_im, full_re, full_im)

    tile_p = jnp.where(
        lax.rem(iota((states, gp), 1), states) == iota((states, gp), 0), 1.0, 0.0
    )
    widen = jnp.where(
        iota((groups, gp), 1) // states == iota((groups, gp), 0), 1.0, 0.0
    ).astype(f32)
    packed = jnp.concatenate([keep_re, upper_imag, big_re, big_im, full_re, full_im], axis=0)
    spread = dot(packed, tile_p, precision=highest)
    k_re, k_im, b_re, b_im, full_re, full_im = [
        jnp.sum(spread[i * groups : (i + 1) * groups] * widen, axis=0, keepdims=True)
        for i in range(6)
    ]
    tile_p = tile_p.astype(bf16)
    mask_out = iota((chans, gp), 0) // channels == iota((chans, gp), 1) // states

    def wide(value):
        return [
            jnp.where(mask_out, dot(part, tile_p), 0.0).astype(bf16) for part in split(value)
        ]

    copies = jnp.where(
        iota((chans, groups), 0) // channels == iota((chans, groups), 1), 1.0, 0.0
    ).astype(f32)
    f_re, f_im = dot(copies, f_re, precision=highest), dot(copies, f_im, precision=highest)
    bar_re, bar_im = cmul(f_re, f_im, in_re_ref[...], in_im_ref[...])

    row_i, col_i = iota((tokens, tokens), 0), iota((tokens, tokens), 1)
    perm = jnp.where(
        col_i == lax.rem(row_i, SPANS) * span + row_i // SPANS, 1.0, 0.0
    ).astype(bf16)
    x = dot(perm, x_ref[...]).astype(bf16)
    for bar, d_ref in ((bar_re, d_re), (bar_im, d_im)):
        high, low = wide(bar)
        d_ref[...] = dot(x, high) + dot(x, low)
    held = dot(jnp.exp(ret_ref[...]), perm.astype(f32), NT, precision=highest)
    shr[...] = dot(held, widen, TN, precision=highest)

    k_re = jnp.broadcast_to(k_re, (SPANS, gp))
    k_im = jnp.broadcast_to(k_im, (SPANS, gp))

    def advance(j, s_re, s_im):
        at = pl.ds(pl.multiple_of(j * SPANS, SPANS), SPANS)
        m_re, m_im = cmul(k_re, k_im, s_re, s_im)
        shrink = shr[at, :]
        return at, shrink, shrink * m_re + d_re[at, :], shrink * m_im + d_im[at, :]

    def first(j, state):
        s_re, s_im, total = state
        _, shrink, s_re, s_im = advance(j, s_re, s_im)
        return s_re, s_im, total * shrink

    zero = jnp.zeros((SPANS, gp), f32)
    e_re, e_im, total = lax.fori_loop(0, span, first, (zero, zero, zero + 1.0))
    a_re, a_im = total * b_re, total * b_im

    one = jnp.ones((1, gp), f32)
    nil = jnp.zeros((1, gp), f32)
    c_re, c_im, s_re, s_im = one, nil, nil, nil
    entries = []
    for i in range(SPANS):
        entries.append((c_re, c_im, s_re, s_im))
        ar, ai = a_re[i : i + 1], a_im[i : i + 1]
        s_re, s_im = cmul(ar, ai, s_re, s_im)
        s_re, s_im = s_re + e_re[i : i + 1], s_im + e_im[i : i + 1]
        c_re, c_im = cmul(ar, ai, c_re, c_im)
    held_all = total[0:1]
    for i in range(1, SPANS):
        held_all = held_all * total[i : i + 1]
    for i, part in enumerate((held_all, s_re, s_im)):
        carry_out[i : i + 1, :] = part

    def carry_copy(k):
        return pltpu.make_async_remote_copy(
            carry_out, carry_in.at[sp], car_s.at[k], car_r.at[k],
            device_id={"sp": lax.rem(sp + k + 1, n_sp)},
        )

    def carry_start(k):
        @pl.when(sp + k + 1 < n_sp)
        def _():
            carry_copy(k).start()

    def carry_arrived(k):
        @pl.when(sp > k)
        def _():
            carry_copy(k).wait_recv()

    def carry_sent(k):
        @pl.when(sp + k + 1 < n_sp)
        def _():
            carry_copy(k).wait_send()

    repeat(n_sp - 1, carry_start)
    if flood:
        for part in range(1, HALVES):
            hop_start(0, part)
    c_re, c_im, s_re, s_im = [
        jnp.concatenate([entry[i] for entry in entries], axis=0) for i in range(4)
    ]

    o_re, o_im = wide(out_re_ref[...]), wide(out_im_ref[...])
    tile_c = jnp.where(
        lax.rem(iota((channels, chans), 1), channels) == iota((channels, chans), 0), 1.0, 0.0
    ).astype(f32)
    own_group = iota((groups, chans), 1) // channels == iota((groups, chans), 0)
    skip = jnp.where(own_group, dot(skip_ref[...], tile_c, precision=highest), 0.0)
    skip = jnp.sum(skip, axis=0, keepdims=True)

    if flood:
        share(hi, pick_out[pl.ds(pl.multiple_of(hi * LO * cap, LO * cap), LO * cap), :], res_ref)
        hop_pass(0, 0)
    repeat(n_sp - 1, carry_arrived)
    if flood:
        for part in range(1, HALVES):
            hop_pass(0, part)

    def fold(position, state):
        part = carry_in[position]
        n_re, n_im = cmul(part[0:1] * full_re, part[0:1] * full_im, *state)
        return (
            jnp.where(position < sp, n_re + part[1:2], state[0]),
            jnp.where(position < sp, n_im + part[2:3], state[1]),
        )

    state = (nil, nil)
    if n_sp <= 8:
        for position in range(n_sp - 1):
            state = fold(position, state)
    else:
        state = lax.fori_loop(0, n_sp - 1, fold, state)
    m_re, m_im = cmul(c_re, c_im, *state)

    def second(j, state):
        at, _, s_re, s_im = advance(j, *state)
        d_re[at, :] = s_re
        d_im[at, :] = s_im
        return s_re, s_im

    lax.fori_loop(0, span, second, (s_re + m_re, s_im + m_im))

    def read(ref, wide):
        high, low = split(ref[...])
        return dot(high, wide[0], NT) + dot(low, wide[0], NT) + dot(high, wide[1], NT)

    y = read(d_re, o_re) - read(d_im, o_im) + skip * x.astype(f32)
    y = jax.nn.gelu(y).astype(bf16)
    mix_out[...] = dot(perm, y, TN).astype(bf16)

    def mine(index):
        return pl.ds(pl.multiple_of(index * rows, rows), rows)

    mixes = []
    for k in range(n_tp - 1):
        peer = lax.rem(tp + k + 1, n_tp)
        mixes.append(
            pltpu.make_async_remote_copy(
                mix_out.at[mine(peer)], mix_in.at[tp], mix_s.at[k], mix_r.at[k],
                device_id={"tp": peer},
            )
        )
        mixes[-1].start()
    for copy in proj_far[PROJ_FIRST:]:
        copy.start()
    mix_in[tp] = mix_out[mine(tp), :]
    if flood:
        repeat(line - 1, lambda k: pick_copy(k).wait_recv())
        hop_pass(1, 0)
        share_line(1)
    for copy in mixes:
        copy.wait_recv()

    total_chans = n_tp * chans
    for part in range(n_tp):
        y_out[:, :, part * chans : (part + 1) * chans] = (
            dot(chosen, mix_in[part]).astype(bf16).reshape(n_sp, cap, chans)
        )

    take = BATCH_ROWS // cap
    batches = n_sp // take
    home = sp // take

    def batch_of(i):
        return lax.rem(home + batches // 2 + i, batches) if batches > 1 else 0

    def others(i, body):
        base = batch_of(i) * take

        def one(j):
            peer = base + j

            @pl.when(peer != sp)
            def _():
                body(peer)

        repeat(take, one)

    def y_copy(peer, source):
        return pltpu.make_async_remote_copy(
            y_out.at[peer], y_in.at[source], y_s.at[peer], y_r.at[source], device_id={"sp": peer}
        )

    repeat(batches, lambda i: others(i, lambda peer: y_copy(peer, sp).start()))
    y_in[sp] = y_out[sp]

    if flood:
        for part in range(1, HALVES):
            hop_pass(1, part)
        share_line(2)
        for step in range(2, line - 1):
            for part in range(HALVES):
                hop_pass(step, part)
            share_line(step + 1)
    for i in range(PROJ_CHUNKS):
        proj_far[i].wait_recv()
        proj_fwd[i].start()
    own.wait()
    proj_near.wait_recv()
    for copy in proj_fwd:
        copy.wait_recv()
    if flood:
        for owner in range(line):
            res_copy(owner).wait_recv()
    else:
        repeat(n_sp - 1, lambda k: send_res(k).wait_recv())
    for copy in loads[1:]:
        copy.wait()

    def hidden_of(y, scaled_ref, acc_ref, residual_of):
        squares = jnp.sum(y * y, axis=1, keepdims=True)
        scaled_ref[...] = (y * gain_ref[...]).astype(bf16)
        scale = lax.rsqrt(squares / total_chans + 1e-06)

        def project(cols):
            weights = proj_all[:, :, cols].reshape(total_chans, 256)
            part = dot(scaled_ref[...], weights)
            acc_ref[:, cols] = deep_alpha * residual_of(cols).astype(f32) + part * scale

        every(width, 256, project)
        return layer_norm(acc_ref[...], mix_gain_ref[...]).astype(bf16)

    def back_copy(peer, source):
        return pltpu.make_async_remote_copy(
            ret_out.at[peer], ret_in.at[source], back_s.at[peer], back_r.at[source],
            device_id={"sp": peer},
        )

    def expert(i):
        base = batch_of(i) * take
        these = pl.ds(base, take)
        others(i, lambda peer: y_copy(peer, peer).wait_recv())
        y = y_in[these].reshape(BATCH_ROWS, total_chans).astype(f32)
        hid_b[...] = hidden_of(
            y, scaled_v, acc_b, lambda cols: res_in[these, :, cols].reshape(BATCH_ROWS, 256)
        )
        gate, up = dot(hid_b[...], gate_v[...]), dot(hid_b[...], up_v[...])
        active = (gate * jax.nn.sigmoid(gate) * up).astype(bf16)

        def produce(cols):
            ret_out[these, :, cols] = (
                dot(active, down_v[:, cols]).astype(bf16).reshape(take, cap, 256)
            )

        every(width, 256, produce)
        others(i, lambda peer: back_copy(peer, sp).start())

    repeat(batches, expert)
    ret_in[sp] = ret_out[sp]
    y = jnp.concatenate([mix_in[part].astype(f32) for part in range(n_tp)], axis=1)
    hid[...] = hidden_of(y, scaled_v.at[pl.ds(0, rows)], acc, lambda cols: res_ref[:, cols])
    repeat(batches, lambda i: others(i, lambda peer: back_copy(peer, peer).wait_recv()))

    def combine(cols):
        got = ret_in[:, :, cols].reshape(slots, 256)
        acc[:, cols] = (
            deep_alpha * hid[:, cols].astype(f32) + dot(w_high, got, TN) + dot(w_low, got, TN)
        )

    every(width, 256, combine)
    o_ref[...] = layer_norm(acc[...], final_gain_ref[...]).astype(bf16)

    for copy in proj_far + [proj_near] + proj_fwd + mixes:
        copy.wait_send()
    repeat(n_sp - 1, carry_sent)
    if flood:
        repeat(line - 1, lambda k: pick_copy(k).wait_send())
        for step in range(line - 1):
            for part in range(HALVES):
                hop_sent(step, part)
        for owner in range(line):
            res_copy(owner).wait_send()
    else:
        repeat(n_sp - 1, lambda k: send_res(k).wait_send())
    repeat(batches, lambda i: others(i, lambda peer: y_copy(peer, sp).wait_send()))
    repeat(batches, lambda i: others(i, lambda peer: back_copy(peer, sp).wait_send()))


def local(
    mixer_input, retention, decay_real, decay_freq, log_step, input_real, input_imag,
    readout_real, readout_imaginary, skip_weight, norm_gain, projection, residual, mix_gain,
    routes, route_weight, expert_gate, expert_up, expert_down, final_gain,
):
    n_sp, n_tp = lax.axis_size("sp"), lax.axis_size("tp")
    tokens, chans = mixer_input.shape
    groups, states, channels = input_real.shape
    gp, rows, width = groups * states, residual.shape[0], residual.shape[1]
    cap = -(-max(2, 2 * rows * PICKS // n_sp) // 16) * 16
    hidden, line = expert_gate.shape[2], n_sp // LO

    def compact(value):
        return jnp.swapaxes(value, 1, 2).reshape(chans, states)

    small = (
        mixer_input, retention, decay_real, decay_freq, log_step[None, :], skip_weight,
        norm_gain[None, :], compact(input_real), compact(input_imag),
        readout_real.reshape(chans, states), readout_imaginary.reshape(chans, states),
        residual, mix_gain[None, :], routes.T, route_weight.T, final_gain[None, :],
    )
    vmem = pl.BlockSpec(memory_space=pltpu.VMEM)
    anywhere = pl.BlockSpec(memory_space=pl.ANY)
    dma = pltpu.SemaphoreType.DMA
    return pl.pallas_call(
        functools.partial(kernel, n_sp, n_tp, groups, channels, states, cap),
        out_shape=jax.ShapeDtypeStruct((rows, width), bf16),
        in_specs=[anywhere] * (len(small) + 4),
        out_specs=vmem,
        scratch_shapes=[pltpu.VMEM(value.shape, value.dtype) for value in small]
        + [
            pltpu.VMEM((tokens, gp), f32),
            pltpu.VMEM((tokens, gp), f32),
            pltpu.VMEM((tokens, gp), f32),
            pltpu.VMEM((3, gp), f32),
            pltpu.VMEM((n_sp, 3, gp), f32),
            pltpu.VMEM((tokens, chans), bf16),
            pltpu.VMEM((n_tp, rows, chans), bf16),
            pltpu.VMEM((n_tp,) + projection.shape, bf16),
            pltpu.VMEM((width, hidden), bf16),
            pltpu.VMEM((width, hidden), bf16),
            pltpu.VMEM((hidden, width), bf16),
            pltpu.VMEM((rows, width), f32),
            pltpu.VMEM((rows, width), bf16),
            pltpu.VMEM((BATCH_ROWS, n_tp * chans), bf16),
            pltpu.VMEM((BATCH_ROWS, width), f32),
            pltpu.VMEM((BATCH_ROWS, width), bf16),
            pltpu.VMEM((n_sp * cap, rows), bf16),
            pltpu.VMEM((line, LO * cap, rows), bf16),
            pltpu.VMEM((line, rows, width) if n_sp <= 8 else (1, 16, 128), bf16),
            pltpu.VMEM((n_sp, cap, width), bf16),
            pltpu.VMEM((n_sp, cap, width), bf16),
            pltpu.VMEM((n_sp, cap, n_tp * chans), bf16),
            pltpu.VMEM((n_sp, cap, n_tp * chans), bf16),
            pltpu.VMEM((n_sp, cap, width), bf16),
            pltpu.VMEM((n_sp, cap, width), bf16),
            dma((len(small),)), dma((4,)),
            dma((n_sp,)), dma((n_sp,)),
            dma((n_tp,)), dma((n_tp,)),
            dma((PROJ_CHUNKS + 1,)), dma((PROJ_CHUNKS + 1,)),
            dma((PROJ_CHUNKS,)), dma((PROJ_CHUNKS,)),
            dma((line,)), dma((line,)),
            dma((line * HALVES,)), dma((line * HALVES,)),
            dma((line * HALVES,)), dma((line * HALVES,)),
            dma((n_sp,)), dma((n_sp,)),
            dma((n_sp,)), dma((n_sp,)),
            dma((n_sp,)), dma((n_sp,)),
        ],
        compiler_params=pltpu.CompilerParams(
            collective_id=0, has_side_effects=True, vmem_limit_bytes=60 * 1024 * 1024
        ),
    )(
        *small,
        projection, expert_gate, expert_up, expert_down,
    )


def solution(mesh):
    in_specs = (
        P("sp", "tp"),
        P("tp", "sp"),
        P("tp", None),
        P("tp", None),
        P("tp"),
        P("tp", None, None),
        P("tp", None, None),
        P("tp", None, None),
        P("tp", None, None),
        P("tp", None),
        P(),
        P("tp", None),
        P(("sp", "tp"), None),
        P(),
        P(("sp", "tp"), None),
        P(("sp", "tp"), None),
        P("sp", None, None),
        P("sp", None, None),
        P("sp", None, None),
        P(),
    )
    out_specs = P(("sp", "tp"), None)
    return jax.shard_map(local, mesh=mesh, in_specs=in_specs, out_specs=out_specs, check_vma=False)
```

```python
import functools

import jax
import jax.numpy as jnp
from jax import lax
from jax.experimental import pallas as pl
from jax.experimental.pallas import tpu as pltpu
from jax.sharding import PartitionSpec as P

PICKS = 2
SPANS = 8
deep_alpha = 2.0**0.25
f32, bf16 = jnp.float32, jnp.bfloat16
highest = lax.Precision.HIGHEST
NT = (((1,), (1,)), ((), ()))
TN = (((0,), (0,)), ((), ()))
PROJ_CHUNKS = 8
PROJ_RELAY = 1
PROJ_FIRST = 1
PROJ_NEXT = 2
EARLY = 2
LO = 2
PIECES = 4
BATCH_ROWS = 128


def dot(a, b, dims=None, precision=None):
    dims = dims or (((1,), (0,)), ((), ()))
    return lax.dot_general(a, b, dims, precision=precision, preferred_element_type=f32)


def split(value):
    high = value.astype(bf16)
    return high, (value - high.astype(f32)).astype(bf16)


def iota(shape, dim):
    return lax.broadcasted_iota(jnp.int32, shape, dim)


def layer_norm(values, scales):
    centered = values - jnp.mean(values, axis=-1, keepdims=True)
    variance = jnp.mean(centered * centered, axis=-1, keepdims=True)
    return centered * lax.rsqrt(variance + 1e-05) * scales


def cmul(ar, ai, br, bi):
    return ar * br - ai * bi, ar * bi + ai * br


def expm1(value, grown):
    series = value * 0.125 + 1.0
    for k in range(7, 1, -1):
        series = series * value * (1.0 / k) + 1.0
    return jnp.where(value > -0.4, series * value, grown - 1.0)


def repeat(count, body):
    if count <= 8:
        for k in range(count):
            body(k)
    else:
        lax.fori_loop(0, count, lambda k, c: (body(k), c)[1], 0)


def kernel(
    n_sp, n_tp, groups, channels, states, cap,
    x_hbm, ret_hbm, real_hbm, freq_hbm, step_hbm, skip_hbm, gain_hbm, in_re_hbm, in_im_hbm,
    out_re_hbm, out_im_hbm, res_hbm, mix_gain_hbm, routes_hbm, rw_hbm, final_gain_hbm,
    proj_ref, gate_ref, up_ref, down_ref,
    o_ref,
    x_ref, ret_ref, real_ref, freq_ref, step_ref, skip_ref, gain_ref, in_re_ref, in_im_ref,
    out_re_ref, out_im_ref, res_ref, mix_gain_ref, routes_ref, rw_ref, final_gain_ref,
    d_re, d_im, shr, carry_out, carry_in, mix_out, mix_in, proj_all, gate_v, up_v, down_v,
    acc, hid, scaled_v, acc_b, hid_b, pick_out, pick_in, raw, res_out, res_in, y_out, y_in,
    ret_out, ret_in,
    in_sem, w_sem, car_s, car_r, mix_s, mix_r, prj_s, prj_r, fwd_s, fwd_r,
    rel_s, pick_s, pick_r, raw_s, raw_r, via_s, res_s, res_r, y_s, y_r, back_s, back_r,
):
    sp, tp = lax.axis_index("sp"), lax.axis_index("tp")
    tokens, chans = x_ref.shape
    gp = groups * states
    span = tokens // SPANS
    rows = tokens // n_tp
    width = o_ref.shape[1]

    small = (
        (step_hbm, step_ref), (real_hbm, real_ref), (freq_hbm, freq_ref), (in_re_hbm, in_re_ref),
        (in_im_hbm, in_im_ref), (x_hbm, x_ref), (ret_hbm, ret_ref), (skip_hbm, skip_ref),
        (out_re_hbm, out_re_ref), (out_im_hbm, out_im_ref), (gain_hbm, gain_ref),
        (routes_hbm, routes_ref), (rw_hbm, rw_ref), (res_hbm, res_ref),
        (mix_gain_hbm, mix_gain_ref), (final_gain_hbm, final_gain_ref),
    )
    fetches = [
        pltpu.make_async_copy(src, dst, in_sem.at[i]) for i, (src, dst) in enumerate(small)
    ]
    for fetch in fetches:
        fetch.start()

    barrier = pltpu.get_barrier_semaphore()

    def greet_sp(k):
        pl.semaphore_signal(barrier, inc=1, device_id={"sp": lax.rem(sp + k + 1, n_sp)})

    def greet_tp(k):
        pl.semaphore_signal(barrier, inc=1, device_id={"tp": lax.rem(tp + k + 1, n_tp)})

    repeat(n_sp - 1, greet_sp)
    repeat(n_tp - 1, greet_tp)

    own = pltpu.make_async_copy(proj_ref, proj_all.at[tp], w_sem.at[0])
    own.start()
    loads = [own]
    for i, (src, dst) in enumerate(((gate_ref, gate_v), (up_ref, up_v), (down_ref, down_v))):
        loads.append(pltpu.make_async_copy(src.at[0], dst, w_sem.at[i + 1]))
        loads[-1].start()
    pl.semaphore_wait(barrier, n_sp - 1 + n_tp - 1)

    depth = proj_ref.shape[0] // PROJ_CHUNKS
    near = tp + 1 - 2 * lax.rem(tp, 2)
    far = lax.rem(tp + 2, n_tp)
    hi, lo = sp // LO, lax.rem(sp, LO)
    line = n_sp // LO
    flood = n_sp == 8

    def piece(i):
        return pl.ds(i * depth, depth)

    direct = PROJ_CHUNKS - LO * PROJ_RELAY
    relayed = [direct + PROJ_RELAY * lo + i for i in range(PROJ_RELAY)]
    foreign = [direct + PROJ_RELAY * (1 - lo) + i for i in range(PROJ_RELAY)]
    sent = relayed + list(range(direct))

    def far_copy(c):
        return pltpu.make_async_remote_copy(
            proj_ref.at[piece(c)], proj_all.at[tp, piece(c)], prj_s.at[c], prj_r.at[c],
            device_id={"tp": far},
        )

    def far_chunk(c):
        return proj_all.at[far, piece(c)]

    def relay_copy(c):
        return pltpu.make_async_remote_copy(
            far_chunk(c), far_chunk(c), rel_s.at[c], prj_r.at[c],
            device_id={"sp": hi * LO + 1 - lo},
        )

    def near_copy(c):
        return pltpu.make_async_remote_copy(
            far_chunk(c), far_chunk(c), fwd_s.at[c], fwd_r.at[c], device_id={"tp": near},
        )

    proj_near = pltpu.make_async_remote_copy(
        proj_ref, proj_all.at[tp], prj_s.at[PROJ_CHUNKS], prj_r.at[PROJ_CHUNKS],
        device_id={"tp": near},
    )
    for c in sent[: PROJ_RELAY + PROJ_FIRST]:
        far_copy(c).start()
    following = sent[PROJ_RELAY + PROJ_FIRST : PROJ_RELAY + PROJ_FIRST + PROJ_NEXT]

    @pl.when(hi >= line // 2)
    def _():
        for c in following:
            far_copy(c).start()


    for fetch in fetches:
        fetch.wait()

    slots = n_sp * cap
    expert_of = iota((slots, rows), 0) // cap
    hit0 = routes_ref[0:1, :] == expert_of
    hit1 = routes_ref[1:2, :] == expert_of
    member = jnp.where(hit0 | hit1, 1.0, 0.0)
    upper = jnp.where(iota((rows, rows), 0) < iota((rows, rows), 1), 1.0, 0.0).astype(bf16)
    place = dot(member.astype(bf16), upper)
    wanted = lax.rem(iota((slots, rows), 0), cap).astype(f32)
    chosen = jnp.where(place == wanted, member, 0.0)
    weight = chosen * jnp.where(hit0, rw_ref[0:1, :], rw_ref[1:2, :])
    chosen = chosen.astype(bf16)
    w_high, w_low = split(weight)

    def every(count, width, body):
        if flood:
            for i in range(count // width):
                body(pl.ds(i * width, width))
            return

        def step(i, c):
            body(pl.ds(pl.multiple_of(i * width, width), width))
            return c

        lax.fori_loop(0, count // width, step, 0)

    piece_rows = rows // PIECES
    mate = hi + 1 - 2 * lax.rem(hi, 2)
    gate_node = 2 - hi // 2
    is_gate = (hi == 1) | (hi == 2)
    beyond = [gate_node, 3 * (1 - hi // 2)]

    def pick_copy(k):
        peer = lax.rem(hi + k + 1, line)
        return pltpu.make_async_remote_copy(
            pick_out.at[pl.ds(pl.multiple_of(peer * LO * cap, LO * cap), LO * cap)],
            pick_in.at[hi], pick_s.at[k], pick_r.at[k], device_id={"sp": peer * LO + lo},
        )

    def rows_at(part):
        return pl.ds(part * piece_rows, piece_rows)

    def raw_copy(kind, part):
        return pltpu.make_async_remote_copy(
            res_ref.at[rows_at(part)], raw.at[hi, rows_at(part)],
            raw_s.at[kind * PIECES + part], raw_r.at[hi * PIECES + part],
            device_id={"sp": (gate_node if kind == 0 else mate) * LO + lo},
        )

    def via_copy(i, part):
        owner = beyond[i]
        return pltpu.make_async_remote_copy(
            raw.at[owner, rows_at(part)], raw.at[owner, rows_at(part)],
            via_s.at[i * PIECES + part], raw_r.at[owner * PIECES + part],
            device_id={"sp": mate * LO + lo},
        )

    def raw_start(kind, part, upward):
        node = mate if kind else gate_node

        @pl.when(node > hi if upward else node < hi)
        def _():
            raw_copy(kind, part).start()

    def raw_arrived(owner, part):
        pltpu.make_async_remote_copy(
            raw.at[owner, rows_at(part)], raw.at[owner, rows_at(part)],
            raw_s.at[part], raw_r.at[owner * PIECES + part], device_id={"sp": mate * LO + lo},
        ).wait_recv()

    def forward(i, part):
        @pl.when(is_gate)
        def _():
            raw_arrived(beyond[i], part)
            via_copy(i, part).start()

    def res_copy(owner):
        return pltpu.make_async_remote_copy(
            res_out.at[owner * LO + 1 - lo], res_in.at[owner * LO + lo],
            res_s.at[owner], res_r.at[owner], device_id={"sp": hi * LO + 1 - lo},
        )

    def share(owner, pick, rows_of):
        def step(cols):
            both = dot(pick, rows_of[:, cols]).astype(bf16).reshape(LO, cap, 256)
            res_out[pl.ds(owner * LO, LO), :, cols] = both

        every(width, 256, step)
        res_in[owner * LO + lo] = res_out[owner * LO + lo]
        res_copy(owner).start()

    def share_line(owner):
        share(owner, pick_in[owner], raw.at[owner])

    def send_res(k):
        peer = lax.rem(sp + k + 1, n_sp)
        return pltpu.make_async_remote_copy(
            res_out.at[peer], res_in.at[sp], res_s.at[k], res_r.at[k], device_id={"sp": peer}
        )

    pick_out[...] = chosen
    if flood:
        repeat(line - 1, lambda k: pick_copy(k).start())
        for kind in (1, 0):
            for part in range(PIECES):
                raw_start(kind, part, False)

        @pl.when(hi > 0)
        def _():
            for part in range(3):
                raw_start(0, part, True)

        for part in range(EARLY):
            raw_start(1, part, True)
        share(hi, pick_out[pl.ds(pl.multiple_of(hi * LO * cap, LO * cap), LO * cap), :], res_ref)
    else:
        def spread_res(cols):
            res_out[:, :, cols] = dot(chosen, res_ref[:, cols]).astype(bf16).reshape(n_sp, cap, 256)

        every(width, 256, spread_res)
        res_in[sp] = res_out[sp]
        repeat(n_sp - 1, lambda k: send_res(k).start())

    eye = iota((groups, groups), 0) == iota((groups, groups), 1)
    stride = jnp.exp(jnp.sum(jnp.where(eye, step_ref[...], 0.0), axis=1, keepdims=True))
    real, freq = real_ref[...], freq_ref[...]
    growth, turning = real * stride, freq * stride
    cosine, sine, half = jnp.cos(turning), jnp.sin(turning), jnp.sin(0.5 * turning)
    size = jnp.exp(growth)
    upper_real = expm1(growth, size) * cosine - 2.0 * half * half
    keep_re, upper_imag = size * cosine, size * sine
    denominator = real * real + freq * freq
    f_re = (upper_real * real + upper_imag * freq) / denominator
    f_im = (upper_imag * real - upper_real * freq) / denominator
    big_re, big_im = keep_re, upper_imag
    for _ in range(span.bit_length() - 1):
        big_re, big_im = cmul(big_re, big_im, big_re, big_im)
    full_re, full_im = big_re, big_im
    for _ in range(SPANS.bit_length() - 1):
        full_re, full_im = cmul(full_re, full_im, full_re, full_im)

    tile_p = jnp.where(
        lax.rem(iota((states, gp), 1), states) == iota((states, gp), 0), 1.0, 0.0
    )
    widen = jnp.where(
        iota((groups, gp), 1) // states == iota((groups, gp), 0), 1.0, 0.0
    ).astype(f32)
    packed = jnp.concatenate([keep_re, upper_imag, big_re, big_im, full_re, full_im], axis=0)
    spread = dot(packed, tile_p, precision=highest)
    k_re, k_im, b_re, b_im, full_re, full_im = [
        jnp.sum(spread[i * groups : (i + 1) * groups] * widen, axis=0, keepdims=True)
        for i in range(6)
    ]
    tile_p = tile_p.astype(bf16)
    mask_out = iota((chans, gp), 0) // channels == iota((chans, gp), 1) // states

    def wide(value):
        return [
            jnp.where(mask_out, dot(part, tile_p), 0.0).astype(bf16) for part in split(value)
        ]

    copies = jnp.where(
        iota((chans, groups), 0) // channels == iota((chans, groups), 1), 1.0, 0.0
    ).astype(f32)
    f_re, f_im = dot(copies, f_re, precision=highest), dot(copies, f_im, precision=highest)
    bar_re, bar_im = cmul(f_re, f_im, in_re_ref[...], in_im_ref[...])

    row_i, col_i = iota((tokens, tokens), 0), iota((tokens, tokens), 1)
    perm = jnp.where(
        col_i == lax.rem(row_i, SPANS) * span + row_i // SPANS, 1.0, 0.0
    ).astype(bf16)
    x = dot(perm, x_ref[...]).astype(bf16)
    for bar, d_ref in ((bar_re, d_re), (bar_im, d_im)):
        high, low = wide(bar)
        d_ref[...] = dot(x, high) + dot(x, low)
    held = jnp.exp(ret_ref[...])
    first_part = held.astype(bf16)
    rest = held - first_part.astype(f32)
    held = dot(jnp.concatenate([first_part, *split(rest)], axis=0), perm, NT).astype(bf16)
    shr[...] = dot(held, jnp.concatenate([widen.astype(bf16)] * 3, axis=0), TN)

    k_re = jnp.broadcast_to(k_re, (SPANS, gp))
    k_im = jnp.broadcast_to(k_im, (SPANS, gp))

    def advance(j, s_re, s_im):
        at = pl.ds(pl.multiple_of(j * SPANS, SPANS), SPANS)
        m_re, m_im = cmul(k_re, k_im, s_re, s_im)
        shrink = shr[at, :]
        return at, shrink, shrink * m_re + d_re[at, :], shrink * m_im + d_im[at, :]

    def first(j, state):
        s_re, s_im, total = state
        _, shrink, s_re, s_im = advance(j, s_re, s_im)
        return s_re, s_im, total * shrink

    zero = jnp.zeros((SPANS, gp), f32)
    e_re, e_im, total = lax.fori_loop(0, span, first, (zero, zero, zero + 1.0))
    a_re, a_im = total * b_re, total * b_im

    one = jnp.ones((1, gp), f32)
    nil = jnp.zeros((1, gp), f32)
    c_re, c_im, s_re, s_im = one, nil, nil, nil
    entries = []
    for i in range(SPANS):
        entries.append((c_re, c_im, s_re, s_im))
        ar, ai = a_re[i : i + 1], a_im[i : i + 1]
        s_re, s_im = cmul(ar, ai, s_re, s_im)
        s_re, s_im = s_re + e_re[i : i + 1], s_im + e_im[i : i + 1]
        c_re, c_im = cmul(ar, ai, c_re, c_im)
    held_all = total[0:1]
    for i in range(1, SPANS):
        held_all = held_all * total[i : i + 1]
    for i, part in enumerate((held_all, s_re, s_im)):
        carry_out[i : i + 1, :] = part

    def carry_copy(k):
        return pltpu.make_async_remote_copy(
            carry_out, carry_in.at[sp], car_s.at[k], car_r.at[k],
            device_id={"sp": lax.rem(sp + k + 1, n_sp)},
        )

    def carry_start(k):
        @pl.when(sp + k + 1 < n_sp)
        def _():
            carry_copy(k).start()

    def carry_arrived(k):
        @pl.when(sp > k)
        def _():
            carry_copy(k).wait_recv()

    def carry_sent(k):
        @pl.when(sp + k + 1 < n_sp)
        def _():
            carry_copy(k).wait_send()

    repeat(n_sp - 1, lambda k: carry_start(n_sp - 2 - k))
    if flood:
        for part in range(EARLY, PIECES):
            raw_start(1, part, True)

        @pl.when(hi > 0)
        def _():
            for part in range(3, PIECES):
                raw_start(0, part, True)

        @pl.when(hi == 0)
        def _():
            for part in range(PIECES):
                raw_copy(0, part).start()

        forward(0, 0)
    c_re, c_im, s_re, s_im = [
        jnp.concatenate([entry[i] for entry in entries], axis=0) for i in range(4)
    ]

    o_re, o_im = wide(out_re_ref[...]), wide(out_im_ref[...])
    tile_c = jnp.where(
        lax.rem(iota((channels, chans), 1), channels) == iota((channels, chans), 0), 1.0, 0.0
    ).astype(f32)
    own_group = iota((groups, chans), 1) // channels == iota((groups, chans), 0)
    skip = jnp.where(own_group, dot(skip_ref[...], tile_c, precision=highest), 0.0)
    skip = jnp.sum(skip, axis=0, keepdims=True)

    if flood:
        forward(0, 1)
    repeat(n_sp - 1, carry_arrived)
    if flood:
        forward(0, 2)
    for c in relayed:
        far_copy(c).wait_recv()
        relay_copy(c).start()
        near_copy(c).start()

    def fold(position, state):
        part = carry_in[position]
        n_re, n_im = cmul(part[0:1] * full_re, part[0:1] * full_im, *state)
        return (
            jnp.where(position < sp, n_re + part[1:2], state[0]),
            jnp.where(position < sp, n_im + part[2:3], state[1]),
        )

    state = (nil, nil)
    if n_sp <= 8:
        for position in range(n_sp - 1):
            state = fold(position, state)
    else:
        state = lax.fori_loop(0, n_sp - 1, fold, state)
    m_re, m_im = cmul(c_re, c_im, *state)

    def second(j, state):
        at, _, s_re, s_im = advance(j, *state)
        d_re[at, :] = s_re
        d_im[at, :] = s_im
        return s_re, s_im

    lax.fori_loop(0, span, second, (s_re + m_re, s_im + m_im))

    def read(ref, wide):
        high, low = split(ref[...])
        return dot(high, wide[0], NT) + dot(low, wide[0], NT) + dot(high, wide[1], NT)

    y = read(d_re, o_re) - read(d_im, o_im) + skip * x.astype(f32)
    y = jax.nn.gelu(y).astype(bf16)
    mix_out[...] = dot(perm, y, TN).astype(bf16)

    def mine(index):
        return pl.ds(pl.multiple_of(index * rows, rows), rows)

    mixes = []
    for k in range(n_tp - 1):
        peer = lax.rem(tp + k + 1, n_tp)
        mixes.append(
            pltpu.make_async_remote_copy(
                mix_out.at[mine(peer)], mix_in.at[tp], mix_s.at[k], mix_r.at[k],
                device_id={"tp": peer},
            )
        )
        mixes[-1].start()

    @pl.when(hi < line // 2)
    def _():
        for c in following:
            far_copy(c).start()

    for c in sent[PROJ_RELAY + PROJ_FIRST + PROJ_NEXT :]:
        far_copy(c).start()
    proj_near.start()
    mix_in[tp] = mix_out[mine(tp), :]
    if flood:
        forward(0, 3)
        forward(1, 0)
        repeat(line - 1, lambda k: pick_copy(k).wait_recv())
        for part in range(PIECES):
            raw_arrived(mate, part)
        share_line(mate)
        forward(1, 1)
    for copy in mixes:
        copy.wait_recv()

    total_chans = n_tp * chans
    for part in range(n_tp):
        y_out[:, :, part * chans : (part + 1) * chans] = (
            dot(chosen, mix_in[part]).astype(bf16).reshape(n_sp, cap, chans)
        )

    take = BATCH_ROWS // cap
    batches = n_sp // take
    home = sp // take

    def batch_of(i):
        return lax.rem(home + i, batches) if batches > 1 else 0

    def others(i, body, backward=False):
        base = batch_of(i) * take

        def one(j):
            peer = base + (take - 1 - j if backward else j)

            @pl.when(peer != sp)
            def _():
                body(peer)

        repeat(take, one)

    def y_copy(peer, source):
        return pltpu.make_async_remote_copy(
            y_out.at[peer], y_in.at[source], y_s.at[peer], y_r.at[source], device_id={"sp": peer}
        )

    def y_start(i):
        outward = home < batches // 2

        @pl.when(outward)
        def _():
            others(i, lambda peer: y_copy(peer, sp).start(), True)

        @pl.when(~outward)
        def _():
            others(i, lambda peer: y_copy(peer, sp).start())

    repeat(batches, lambda i: y_start(batches - 1 - i))
    y_in[sp] = y_out[sp]

    def project_arrived(chunks):
        for c in chunks:
            far_copy(c).wait_recv()
            near_copy(c).start()

    def far_share(i):
        @pl.when(~is_gate)
        def _():
            for part in range(PIECES):
                raw_arrived(beyond[i], part)

        share_line(beyond[i])

    if flood:
        far_share(0)
        forward(1, 2)
        forward(1, 3)

        @pl.when(is_gate)
        def _():
            far_share(1)

        project_arrived(list(range(direct)) + foreign)

        @pl.when(~is_gate)
        def _():
            far_share(1)

    else:
        project_arrived(list(range(direct)) + foreign)
    own.wait()
    proj_near.wait_recv()
    for c in range(PROJ_CHUNKS):
        near_copy(c).wait_recv()
    if flood:
        for owner in range(line):
            res_copy(owner).wait_recv()
    else:
        repeat(n_sp - 1, lambda k: send_res(k).wait_recv())
    for copy in loads[1:]:
        copy.wait()

    def hidden_of(y, scaled_ref, acc_ref, residual_of):
        squares = jnp.sum(y * y, axis=1, keepdims=True)
        scaled_ref[...] = (y * gain_ref[...]).astype(bf16)
        scale = lax.rsqrt(squares / total_chans + 1e-06)

        def project(cols):
            weights = proj_all[:, :, cols].reshape(total_chans, 256)
            part = dot(scaled_ref[...], weights)
            acc_ref[:, cols] = deep_alpha * residual_of(cols).astype(f32) + part * scale

        every(width, 256, project)
        return layer_norm(acc_ref[...], mix_gain_ref[...]).astype(bf16)

    def back_copy(peer, source):
        return pltpu.make_async_remote_copy(
            ret_out.at[peer], ret_in.at[source], back_s.at[peer], back_r.at[source],
            device_id={"sp": peer},
        )

    def expert(i):
        base = batch_of(i) * take
        these = pl.ds(base, take)
        others(i, lambda peer: y_copy(peer, peer).wait_recv())
        y = y_in[these].reshape(BATCH_ROWS, total_chans).astype(f32)
        hid_b[...] = hidden_of(
            y, scaled_v, acc_b, lambda cols: res_in[these, :, cols].reshape(BATCH_ROWS, 256)
        )
        gate, up = dot(hid_b[...], gate_v[...]), dot(hid_b[...], up_v[...])
        active = (gate * jax.nn.sigmoid(gate) * up).astype(bf16)

        def produce(cols):
            ret_out[these, :, cols] = (
                dot(active, down_v[:, cols]).astype(bf16).reshape(take, cap, 256)
            )

        every(width, 256, produce)
        others(i, lambda peer: back_copy(peer, sp).start())

    repeat(batches, expert)
    ret_in[sp] = ret_out[sp]
    y = jnp.concatenate([mix_in[part].astype(f32) for part in range(n_tp)], axis=1)
    hid[...] = hidden_of(y, scaled_v.at[pl.ds(0, rows)], acc, lambda cols: res_ref[:, cols])
    repeat(batches, lambda i: others(i, lambda peer: back_copy(peer, peer).wait_recv()))

    def combine(cols):
        got = ret_in[:, :, cols].reshape(slots, 256)
        acc[:, cols] = (
            deep_alpha * hid[:, cols].astype(f32) + dot(w_high, got, TN) + dot(w_low, got, TN)
        )

    every(width, 256, combine)
    o_ref[...] = layer_norm(acc[...], final_gain_ref[...]).astype(bf16)

    for c in sent:
        far_copy(c).wait_send()
    for c in relayed:
        relay_copy(c).wait_send()
    for c in range(PROJ_CHUNKS):
        near_copy(c).wait_send()
    for copy in [proj_near] + mixes:
        copy.wait_send()
    repeat(n_sp - 1, carry_sent)
    if flood:
        repeat(line - 1, lambda k: pick_copy(k).wait_send())
        for part in range(PIECES):
            for kind in range(2):
                raw_copy(kind, part).wait_send()

        @pl.when(is_gate)
        def _():
            for part in range(PIECES):
                for i in range(2):
                    via_copy(i, part).wait_send()

        for owner in range(line):
            res_copy(owner).wait_send()
    else:
        repeat(n_sp - 1, lambda k: send_res(k).wait_send())
    repeat(batches, lambda i: others(i, lambda peer: y_copy(peer, sp).wait_send()))
    repeat(batches, lambda i: others(i, lambda peer: back_copy(peer, sp).wait_send()))


def local(
    mixer_input, retention, decay_real, decay_freq, log_step, input_real, input_imag,
    readout_real, readout_imaginary, skip_weight, norm_gain, projection, residual, mix_gain,
    routes, route_weight, expert_gate, expert_up, expert_down, final_gain,
):
    n_sp, n_tp = lax.axis_size("sp"), lax.axis_size("tp")
    tokens, chans = mixer_input.shape
    groups, states, channels = input_real.shape
    gp, rows, width = groups * states, residual.shape[0], residual.shape[1]
    cap = -(-max(2, 2 * rows * PICKS // n_sp) // 16) * 16
    hidden, line = expert_gate.shape[2], n_sp // LO

    def compact(value):
        return jnp.swapaxes(value, 1, 2).reshape(chans, states)

    small = (
        mixer_input, retention, decay_real, decay_freq, log_step[None, :], skip_weight,
        norm_gain[None, :], compact(input_real), compact(input_imag),
        readout_real.reshape(chans, states), readout_imaginary.reshape(chans, states),
        residual, mix_gain[None, :], routes.T, route_weight.T, final_gain[None, :],
    )
    vmem = pl.BlockSpec(memory_space=pltpu.VMEM)
    anywhere = pl.BlockSpec(memory_space=pl.ANY)
    dma = pltpu.SemaphoreType.DMA
    return pl.pallas_call(
        functools.partial(kernel, n_sp, n_tp, groups, channels, states, cap),
        out_shape=jax.ShapeDtypeStruct((rows, width), bf16),
        in_specs=[anywhere] * (len(small) + 4),
        out_specs=vmem,
        scratch_shapes=[pltpu.VMEM(value.shape, value.dtype) for value in small]
        + [
            pltpu.VMEM((tokens, gp), f32),
            pltpu.VMEM((tokens, gp), f32),
            pltpu.VMEM((tokens, gp), f32),
            pltpu.VMEM((3, gp), f32),
            pltpu.VMEM((n_sp, 3, gp), f32),
            pltpu.VMEM((tokens, chans), bf16),
            pltpu.VMEM((n_tp, rows, chans), bf16),
            pltpu.VMEM((n_tp,) + projection.shape, bf16),
            pltpu.VMEM((width, hidden), bf16),
            pltpu.VMEM((width, hidden), bf16),
            pltpu.VMEM((hidden, width), bf16),
            pltpu.VMEM((rows, width), f32),
            pltpu.VMEM((rows, width), bf16),
            pltpu.VMEM((BATCH_ROWS, n_tp * chans), bf16),
            pltpu.VMEM((BATCH_ROWS, width), f32),
            pltpu.VMEM((BATCH_ROWS, width), bf16),
            pltpu.VMEM((n_sp * cap, rows), bf16),
            pltpu.VMEM((line, LO * cap, rows), bf16),
            pltpu.VMEM((line, rows, width) if n_sp == 8 else (1, 16, 128), bf16),
            pltpu.VMEM((n_sp, cap, width), bf16),
            pltpu.VMEM((n_sp, cap, width), bf16),
            pltpu.VMEM((n_sp, cap, n_tp * chans), bf16),
            pltpu.VMEM((n_sp, cap, n_tp * chans), bf16),
            pltpu.VMEM((n_sp, cap, width), bf16),
            pltpu.VMEM((n_sp, cap, width), bf16),
            dma((len(small),)), dma((4,)),
            dma((n_sp,)), dma((n_sp,)),
            dma((n_tp,)), dma((n_tp,)),
            dma((PROJ_CHUNKS + 1,)), dma((PROJ_CHUNKS + 1,)),
            dma((PROJ_CHUNKS,)), dma((PROJ_CHUNKS,)),
            dma((PROJ_CHUNKS,)), dma((line,)), dma((line,)),
            dma((2 * PIECES,)), dma((line * PIECES,)), dma((2 * PIECES,)),
            dma((n_sp,)), dma((n_sp,)),
            dma((n_sp,)), dma((n_sp,)),
            dma((n_sp,)), dma((n_sp,)),
        ],
        compiler_params=pltpu.CompilerParams(
            collective_id=0, has_side_effects=True, vmem_limit_bytes=60 * 1024 * 1024
        ),
    )(
        *small,
        projection, expert_gate, expert_up, expert_down,
    )


def solution(mesh):
    in_specs = (
        P("sp", "tp"),
        P("tp", "sp"),
        P("tp", None),
        P("tp", None),
        P("tp"),
        P("tp", None, None),
        P("tp", None, None),
        P("tp", None, None),
        P("tp", None, None),
        P("tp", None),
        P(),
        P("tp", None),
        P(("sp", "tp"), None),
        P(),
        P(("sp", "tp"), None),
        P(("sp", "tp"), None),
        P("sp", None, None),
        P("sp", None, None),
        P("sp", None, None),
        P(),
    )
    out_specs = P(("sp", "tp"), None)
    return jax.shard_map(local, mesh=mesh, in_specs=in_specs, out_specs=out_specs, check_vma=False)
```

```python
import functools

import jax
import jax.numpy as jnp
from jax import lax
from jax.experimental import pallas as pl
from jax.experimental.pallas import tpu as pltpu
from jax.sharding import PartitionSpec as P

PICKS = 2
SPANS = 8
deep_alpha = 2.0**0.25
f32, bf16 = jnp.float32, jnp.bfloat16
highest = lax.Precision.HIGHEST
NT = (((1,), (1,)), ((), ()))
TN = (((0,), (0,)), ((), ()))
PROJ_CHUNKS = 8
PROJ_RELAY = 1
PROJ_FIRST = 1
PROJ_NEXT = 2
EARLY = 2
DIRECT_SHARE = 2
LO = 2
PIECES = 4
BATCH_ROWS = 128


def dot(a, b, dims=None, precision=None):
    dims = dims or (((1,), (0,)), ((), ()))
    return lax.dot_general(a, b, dims, precision=precision, preferred_element_type=f32)


def split(value):
    high = value.astype(bf16)
    return high, (value - high.astype(f32)).astype(bf16)


def iota(shape, dim):
    return lax.broadcasted_iota(jnp.int32, shape, dim)


def layer_norm(values, scales):
    centered = values - jnp.mean(values, axis=-1, keepdims=True)
    variance = jnp.mean(centered * centered, axis=-1, keepdims=True)
    return centered * lax.rsqrt(variance + 1e-05) * scales


def cmul(ar, ai, br, bi):
    return ar * br - ai * bi, ar * bi + ai * br


def expm1(value, grown):
    series = value * 0.125 + 1.0
    for k in range(7, 1, -1):
        series = series * value * (1.0 / k) + 1.0
    return jnp.where(value > -0.4, series * value, grown - 1.0)


def repeat(count, body):
    if count <= 8:
        for k in range(count):
            body(k)
    else:
        lax.fori_loop(0, count, lambda k, c: (body(k), c)[1], 0)


def kernel(
    n_sp, n_tp, groups, channels, states, cap,
    x_hbm, ret_hbm, real_hbm, freq_hbm, step_hbm, skip_hbm, gain_hbm, in_re_hbm, in_im_hbm,
    out_re_hbm, out_im_hbm, res_hbm, mix_gain_hbm, routes_hbm, rw_hbm, final_gain_hbm,
    proj_ref, gate_ref, up_ref, down_ref,
    o_ref,
    x_ref, ret_ref, real_ref, freq_ref, step_ref, skip_ref, gain_ref, in_re_ref, in_im_ref,
    out_re_ref, out_im_ref, res_ref, mix_gain_ref, routes_ref, rw_ref, final_gain_ref,
    d_re, d_im, shr, carry_out, carry_in, mix_out, mix_in, proj_all, gate_v, up_v, down_v,
    acc, hid, scaled_v, acc_b, hid_b, pick_out, pick_in, raw, res_out, res_in, y_out, y_in,
    ret_out, ret_in, w_out, gate_w, gate_in, gate_out, sum_in,
    in_sem, w_sem, car_s, car_r, mix_s, mix_r, prj_s, prj_r, fwd_s, fwd_r,
    rel_s, pick_s, pick_r, raw_s, raw_r, via_s, res_s, res_r, y_s, y_r, back_s, back_r, gw_s, gw_r, gc_s, gc_r, sum_s, sum_r,
):
    sp, tp = lax.axis_index("sp"), lax.axis_index("tp")
    tokens, chans = x_ref.shape
    gp = groups * states
    span = tokens // SPANS
    rows = tokens // n_tp
    width = o_ref.shape[1]

    small = (
        (step_hbm, step_ref), (real_hbm, real_ref), (freq_hbm, freq_ref), (in_re_hbm, in_re_ref),
        (in_im_hbm, in_im_ref), (x_hbm, x_ref), (ret_hbm, ret_ref), (skip_hbm, skip_ref),
        (out_re_hbm, out_re_ref), (out_im_hbm, out_im_ref), (gain_hbm, gain_ref),
        (routes_hbm, routes_ref), (rw_hbm, rw_ref), (res_hbm, res_ref),
        (mix_gain_hbm, mix_gain_ref), (final_gain_hbm, final_gain_ref),
    )
    fetches = [
        pltpu.make_async_copy(src, dst, in_sem.at[i]) for i, (src, dst) in enumerate(small)
    ]
    for fetch in fetches:
        fetch.start()

    barrier = pltpu.get_barrier_semaphore()

    def greet_sp(k):
        pl.semaphore_signal(barrier, inc=1, device_id={"sp": lax.rem(sp + k + 1, n_sp)})

    def greet_tp(k):
        pl.semaphore_signal(barrier, inc=1, device_id={"tp": lax.rem(tp + k + 1, n_tp)})

    repeat(n_sp - 1, greet_sp)
    repeat(n_tp - 1, greet_tp)

    own = pltpu.make_async_copy(proj_ref, proj_all.at[tp], w_sem.at[0])
    own.start()
    loads = [own]
    for i, (src, dst) in enumerate(((gate_ref, gate_v), (up_ref, up_v), (down_ref, down_v))):
        loads.append(pltpu.make_async_copy(src.at[0], dst, w_sem.at[i + 1]))
        loads[-1].start()
    pl.semaphore_wait(barrier, n_sp - 1 + n_tp - 1)

    depth = proj_ref.shape[0] // PROJ_CHUNKS
    near = tp + 1 - 2 * lax.rem(tp, 2)
    far = lax.rem(tp + 2, n_tp)
    hi, lo = sp // LO, lax.rem(sp, LO)
    line = n_sp // LO
    flood = n_sp == 8

    def piece(i):
        return pl.ds(i * depth, depth)

    direct = PROJ_CHUNKS - LO * PROJ_RELAY
    relayed = [direct + PROJ_RELAY * lo + i for i in range(PROJ_RELAY)]
    foreign = [direct + PROJ_RELAY * (1 - lo) + i for i in range(PROJ_RELAY)]
    sent = relayed + list(range(direct))

    def far_copy(c):
        return pltpu.make_async_remote_copy(
            proj_ref.at[piece(c)], proj_all.at[tp, piece(c)], prj_s.at[c], prj_r.at[c],
            device_id={"tp": far},
        )

    def far_chunk(c):
        return proj_all.at[far, piece(c)]

    def relay_copy(c):
        return pltpu.make_async_remote_copy(
            far_chunk(c), far_chunk(c), rel_s.at[c], prj_r.at[c],
            device_id={"sp": hi * LO + 1 - lo},
        )

    def near_copy(c):
        return pltpu.make_async_remote_copy(
            far_chunk(c), far_chunk(c), fwd_s.at[c], fwd_r.at[c], device_id={"tp": near},
        )

    proj_near = pltpu.make_async_remote_copy(
        proj_ref, proj_all.at[tp], prj_s.at[PROJ_CHUNKS], prj_r.at[PROJ_CHUNKS],
        device_id={"tp": near},
    )
    for c in sent[: PROJ_RELAY + PROJ_FIRST]:
        far_copy(c).start()
    following = sent[PROJ_RELAY + PROJ_FIRST : PROJ_RELAY + PROJ_FIRST + PROJ_NEXT]

    @pl.when(hi >= line // 2)
    def _():
        for c in following:
            far_copy(c).start()


    for fetch in fetches:
        fetch.wait()

    slots = n_sp * cap
    expert_of = iota((slots, rows), 0) // cap
    hit0 = routes_ref[0:1, :] == expert_of
    hit1 = routes_ref[1:2, :] == expert_of
    member = jnp.where(hit0 | hit1, 1.0, 0.0)
    upper = jnp.where(iota((rows, rows), 0) < iota((rows, rows), 1), 1.0, 0.0).astype(bf16)
    place = dot(member.astype(bf16), upper)
    wanted = lax.rem(iota((slots, rows), 0), cap).astype(f32)
    chosen = jnp.where(place == wanted, member, 0.0)
    weight = chosen * jnp.where(hit0, rw_ref[0:1, :], rw_ref[1:2, :])
    chosen = chosen.astype(bf16)
    w_high, w_low = split(weight)

    def every(count, width, body):
        if flood:
            for i in range(count // width):
                body(pl.ds(i * width, width))
            return

        def step(i, c):
            body(pl.ds(pl.multiple_of(i * width, width), width))
            return c

        lax.fori_loop(0, count // width, step, 0)

    piece_rows = rows // PIECES
    mate = hi + 1 - 2 * lax.rem(hi, 2)
    gate_node = 2 - hi // 2
    is_gate = (hi == 1) | (hi == 2)
    beyond = [gate_node, 3 * (1 - hi // 2)]

    def pick_copy(k):
        peer = lax.rem(hi + k + 1, line)
        return pltpu.make_async_remote_copy(
            pick_out.at[pl.ds(pl.multiple_of(peer * LO * cap, LO * cap), LO * cap)],
            pick_in.at[hi], pick_s.at[k], pick_r.at[k], device_id={"sp": peer * LO + lo},
        )

    def rows_at(part):
        return pl.ds(part * piece_rows, piece_rows)

    def raw_copy(kind, part):
        return pltpu.make_async_remote_copy(
            res_ref.at[rows_at(part)], raw.at[hi, rows_at(part)],
            raw_s.at[kind * PIECES + part], raw_r.at[hi * PIECES + part],
            device_id={"sp": (gate_node if kind == 0 else mate) * LO + lo},
        )

    def via_copy(i, part):
        owner = beyond[i]
        return pltpu.make_async_remote_copy(
            raw.at[owner, rows_at(part)], raw.at[owner, rows_at(part)],
            via_s.at[i * PIECES + part], raw_r.at[owner * PIECES + part],
            device_id={"sp": mate * LO + lo},
        )

    def raw_start(kind, part, upward):
        node = mate if kind else gate_node

        @pl.when(node > hi if upward else node < hi)
        def _():
            raw_copy(kind, part).start()

    def raw_arrived(owner, part):
        pltpu.make_async_remote_copy(
            raw.at[owner, rows_at(part)], raw.at[owner, rows_at(part)],
            raw_s.at[part], raw_r.at[owner * PIECES + part], device_id={"sp": mate * LO + lo},
        ).wait_recv()

    def forward(i, part):
        @pl.when(is_gate)
        def _():
            raw_arrived(beyond[i], part)
            via_copy(i, part).start()

    def res_copy(owner):
        return pltpu.make_async_remote_copy(
            res_out.at[owner * LO + 1 - lo], res_in.at[owner * LO + lo],
            res_s.at[owner], res_r.at[owner], device_id={"sp": hi * LO + 1 - lo},
        )

    def share(owner, pick, rows_of):
        def step(cols):
            both = dot(pick, rows_of[:, cols]).astype(bf16).reshape(LO, cap, 256)
            res_out[pl.ds(owner * LO, LO), :, cols] = both

        every(width, 256, step)
        res_in[owner * LO + lo] = res_out[owner * LO + lo]
        res_copy(owner).start()

    def share_line(owner):
        share(owner, pick_in[owner], raw.at[owner])

    def send_res(k):
        peer = lax.rem(sp + k + 1, n_sp)
        return pltpu.make_async_remote_copy(
            res_out.at[peer], res_in.at[sp], res_s.at[k], res_r.at[k], device_id={"sp": peer}
        )

    take = BATCH_ROWS // cap
    batches = n_sp // take
    home = sp // take

    def batch_of(i):
        return lax.rem(home + i, batches) if batches > 1 else 0

    close, apart = home * take, batch_of(1) * take
    keep = width // DIRECT_SHARE if flood else width
    turn = hi // 2
    order = (1 - turn, turn)

    def their_weight():
        slab = pl.ds(pl.multiple_of(apart * cap, BATCH_ROWS), BATCH_ROWS)
        return pltpu.make_async_remote_copy(
            w_out.at[:, slab], gate_w.at[lax.rem(hi, 2)], gw_s.at[0], gw_r.at[lax.rem(hi, 2)],
            device_id={"sp": gate_node * LO + lo},
        )

    def part_copy(t, column, way):
        return pltpu.make_async_remote_copy(
            ret_out.at[apart + LO * t + column, :, pl.ds(keep, width - keep)],
            gate_in.at[t, sp - close], gc_s.at[2 * way + t], gc_r.at[t * take + sp - close],
            device_id={"sp": (1 + turn) * LO + column},
        )

    def part_arrived(t, c):
        pltpu.make_async_remote_copy(
            gate_in.at[t, c], gate_in.at[t, c], gc_s.at[0], gc_r.at[t * take + c],
            device_id={"sp": mate * LO + lo},
        ).wait_recv()

    def sum_copy(t):
        return pltpu.make_async_remote_copy(
            gate_out.at[t], sum_in, sum_s.at[t], sum_r.at[0],
            device_id={"sp": apart + LO * t + lo},
        )

    pick_out[...] = chosen
    w_out[0] = w_high
    w_out[1] = w_low
    if flood:
        repeat(line - 1, lambda k: pick_copy(k).start())
        for kind in (1, 0):
            for part in range(PIECES):
                raw_start(kind, part, False)

        @pl.when(hi > 0)
        def _():
            for part in range(3):
                raw_start(0, part, True)

        for part in range(EARLY):
            raw_start(1, part, True)
        share(hi, pick_out[pl.ds(pl.multiple_of(hi * LO * cap, LO * cap), LO * cap), :], res_ref)
    else:
        def spread_res(cols):
            res_out[:, :, cols] = dot(chosen, res_ref[:, cols]).astype(bf16).reshape(n_sp, cap, 256)

        every(width, 256, spread_res)
        res_in[sp] = res_out[sp]
        repeat(n_sp - 1, lambda k: send_res(k).start())

    eye = iota((groups, groups), 0) == iota((groups, groups), 1)
    stride = jnp.exp(jnp.sum(jnp.where(eye, step_ref[...], 0.0), axis=1, keepdims=True))
    real, freq = real_ref[...], freq_ref[...]
    growth, turning = real * stride, freq * stride
    cosine, sine, half = jnp.cos(turning), jnp.sin(turning), jnp.sin(0.5 * turning)
    size = jnp.exp(growth)
    upper_real = expm1(growth, size) * cosine - 2.0 * half * half
    keep_re, upper_imag = size * cosine, size * sine
    denominator = real * real + freq * freq
    f_re = (upper_real * real + upper_imag * freq) / denominator
    f_im = (upper_imag * real - upper_real * freq) / denominator
    big_re, big_im = keep_re, upper_imag
    for _ in range(span.bit_length() - 1):
        big_re, big_im = cmul(big_re, big_im, big_re, big_im)
    full_re, full_im = big_re, big_im
    for _ in range(SPANS.bit_length() - 1):
        full_re, full_im = cmul(full_re, full_im, full_re, full_im)

    tile_p = jnp.where(
        lax.rem(iota((states, gp), 1), states) == iota((states, gp), 0), 1.0, 0.0
    )
    widen = jnp.where(
        iota((groups, gp), 1) // states == iota((groups, gp), 0), 1.0, 0.0
    ).astype(f32)
    packed = jnp.concatenate([keep_re, upper_imag, big_re, big_im, full_re, full_im], axis=0)
    spread = dot(packed, tile_p, precision=highest)
    k_re, k_im, b_re, b_im, full_re, full_im = [
        jnp.sum(spread[i * groups : (i + 1) * groups] * widen, axis=0, keepdims=True)
        for i in range(6)
    ]
    tile_p = tile_p.astype(bf16)
    mask_out = iota((chans, gp), 0) // channels == iota((chans, gp), 1) // states

    def wide(value):
        return [
            jnp.where(mask_out, dot(part, tile_p), 0.0).astype(bf16) for part in split(value)
        ]

    copies = jnp.where(
        iota((chans, groups), 0) // channels == iota((chans, groups), 1), 1.0, 0.0
    ).astype(f32)
    f_re, f_im = dot(copies, f_re, precision=highest), dot(copies, f_im, precision=highest)
    bar_re, bar_im = cmul(f_re, f_im, in_re_ref[...], in_im_ref[...])

    row_i, col_i = iota((tokens, tokens), 0), iota((tokens, tokens), 1)
    perm = jnp.where(
        col_i == lax.rem(row_i, SPANS) * span + row_i // SPANS, 1.0, 0.0
    ).astype(bf16)
    x = dot(perm, x_ref[...]).astype(bf16)
    for bar, d_ref in ((bar_re, d_re), (bar_im, d_im)):
        high, low = wide(bar)
        d_ref[...] = dot(x, high) + dot(x, low)
    held = jnp.exp(ret_ref[...])
    first_part = held.astype(bf16)
    rest = held - first_part.astype(f32)
    held = dot(jnp.concatenate([first_part, *split(rest)], axis=0), perm, NT).astype(bf16)
    shr[...] = dot(held, jnp.concatenate([widen.astype(bf16)] * 3, axis=0), TN)

    k_re = jnp.broadcast_to(k_re, (SPANS, gp))
    k_im = jnp.broadcast_to(k_im, (SPANS, gp))

    def advance(j, s_re, s_im):
        at = pl.ds(pl.multiple_of(j * SPANS, SPANS), SPANS)
        m_re, m_im = cmul(k_re, k_im, s_re, s_im)
        shrink = shr[at, :]
        return at, shrink, shrink * m_re + d_re[at, :], shrink * m_im + d_im[at, :]

    def first(j, state):
        s_re, s_im, total = state
        _, shrink, s_re, s_im = advance(j, s_re, s_im)
        return s_re, s_im, total * shrink

    zero = jnp.zeros((SPANS, gp), f32)
    e_re, e_im, total = lax.fori_loop(0, span, first, (zero, zero, zero + 1.0))
    a_re, a_im = total * b_re, total * b_im

    one = jnp.ones((1, gp), f32)
    nil = jnp.zeros((1, gp), f32)
    c_re, c_im, s_re, s_im = one, nil, nil, nil
    entries = []
    for i in range(SPANS):
        entries.append((c_re, c_im, s_re, s_im))
        ar, ai = a_re[i : i + 1], a_im[i : i + 1]
        s_re, s_im = cmul(ar, ai, s_re, s_im)
        s_re, s_im = s_re + e_re[i : i + 1], s_im + e_im[i : i + 1]
        c_re, c_im = cmul(ar, ai, c_re, c_im)
    held_all = total[0:1]
    for i in range(1, SPANS):
        held_all = held_all * total[i : i + 1]
    for i, part in enumerate((held_all, s_re, s_im)):
        carry_out[i : i + 1, :] = part

    def carry_copy(k):
        return pltpu.make_async_remote_copy(
            carry_out, carry_in.at[sp], car_s.at[k], car_r.at[k],
            device_id={"sp": lax.rem(sp + k + 1, n_sp)},
        )

    def carry_start(k):
        @pl.when(sp + k + 1 < n_sp)
        def _():
            carry_copy(k).start()

    def carry_arrived(k):
        @pl.when(sp > k)
        def _():
            carry_copy(k).wait_recv()

    def carry_sent(k):
        @pl.when(sp + k + 1 < n_sp)
        def _():
            carry_copy(k).wait_send()

    repeat(n_sp - 1, lambda k: carry_start(n_sp - 2 - k))
    if flood:
        for part in range(EARLY, PIECES):
            raw_start(1, part, True)

        @pl.when(hi > 0)
        def _():
            for part in range(3, PIECES):
                raw_start(0, part, True)

        @pl.when(hi == 0)
        def _():
            for part in range(PIECES):
                raw_copy(0, part).start()

        forward(0, 0)
    c_re, c_im, s_re, s_im = [
        jnp.concatenate([entry[i] for entry in entries], axis=0) for i in range(4)
    ]

    o_re, o_im = wide(out_re_ref[...]), wide(out_im_ref[...])
    tile_c = jnp.where(
        lax.rem(iota((channels, chans), 1), channels) == iota((channels, chans), 0), 1.0, 0.0
    ).astype(f32)
    own_group = iota((groups, chans), 1) // channels == iota((groups, chans), 0)
    skip = jnp.where(own_group, dot(skip_ref[...], tile_c, precision=highest), 0.0)
    skip = jnp.sum(skip, axis=0, keepdims=True)

    if flood:
        forward(0, 1)
    repeat(n_sp - 1, carry_arrived)
    if flood:
        forward(0, 2)
    for c in relayed:
        far_copy(c).wait_recv()
        relay_copy(c).start()
        near_copy(c).start()

    def fold(position, state):
        part = carry_in[position]
        n_re, n_im = cmul(part[0:1] * full_re, part[0:1] * full_im, *state)
        return (
            jnp.where(position < sp, n_re + part[1:2], state[0]),
            jnp.where(position < sp, n_im + part[2:3], state[1]),
        )

    state = (nil, nil)
    if n_sp <= 8:
        for position in range(n_sp - 1):
            state = fold(position, state)
    else:
        state = lax.fori_loop(0, n_sp - 1, fold, state)
    m_re, m_im = cmul(c_re, c_im, *state)

    def second(j, state):
        at, _, s_re, s_im = advance(j, *state)
        d_re[at, :] = s_re
        d_im[at, :] = s_im
        return s_re, s_im

    lax.fori_loop(0, span, second, (s_re + m_re, s_im + m_im))

    def read(ref, wide):
        high, low = split(ref[...])
        return dot(high, wide[0], NT) + dot(low, wide[0], NT) + dot(high, wide[1], NT)

    y = read(d_re, o_re) - read(d_im, o_im) + skip * x.astype(f32)
    y = jax.nn.gelu(y).astype(bf16)
    mix_out[...] = dot(perm, y, TN).astype(bf16)

    def mine(index):
        return pl.ds(pl.multiple_of(index * rows, rows), rows)

    mixes = []
    for k in range(n_tp - 1):
        peer = lax.rem(tp + k + 1, n_tp)
        mixes.append(
            pltpu.make_async_remote_copy(
                mix_out.at[mine(peer)], mix_in.at[tp], mix_s.at[k], mix_r.at[k],
                device_id={"tp": peer},
            )
        )
        mixes[-1].start()

    @pl.when(hi < line // 2)
    def _():
        for c in following:
            far_copy(c).start()

    for c in sent[PROJ_RELAY + PROJ_FIRST + PROJ_NEXT :]:
        far_copy(c).start()
    proj_near.start()
    mix_in[tp] = mix_out[mine(tp), :]
    if flood:
        forward(0, 3)
        forward(1, 0)
        repeat(line - 1, lambda k: pick_copy(k).wait_recv())
        for part in range(PIECES):
            raw_arrived(mate, part)
        share_line(mate)
        forward(1, 1)
    for copy in mixes:
        copy.wait_recv()

    total_chans = n_tp * chans
    for part in range(n_tp):
        y_out[:, :, part * chans : (part + 1) * chans] = (
            dot(chosen, mix_in[part]).astype(bf16).reshape(n_sp, cap, chans)
        )

    def others(i, body, backward=False):
        base = batch_of(i) * take

        def one(j):
            peer = base + (take - 1 - j if backward else j)

            @pl.when(peer != sp)
            def _():
                body(peer)

        repeat(take, one)

    def y_copy(peer, source):
        return pltpu.make_async_remote_copy(
            y_out.at[peer], y_in.at[source], y_s.at[peer], y_r.at[source], device_id={"sp": peer}
        )

    def y_start(i):
        outward = home < batches // 2

        @pl.when(outward)
        def _():
            others(i, lambda peer: y_copy(peer, sp).start(), True)

        @pl.when(~outward)
        def _():
            others(i, lambda peer: y_copy(peer, sp).start())

    repeat(batches, lambda i: y_start(batches - 1 - i))
    y_in[sp] = y_out[sp]

    def project_arrived(chunks):
        for c in chunks:
            far_copy(c).wait_recv()
            near_copy(c).start()

    def far_share(i):
        @pl.when(~is_gate)
        def _():
            for part in range(PIECES):
                raw_arrived(beyond[i], part)

        share_line(beyond[i])

    if flood:
        far_share(0)
        forward(1, 2)
        forward(1, 3)

        @pl.when(is_gate)
        def _():
            far_share(1)

        project_arrived(list(range(direct)) + foreign)

        @pl.when(~is_gate)
        def _():
            far_share(1)

    else:
        project_arrived(list(range(direct)) + foreign)
    own.wait()
    proj_near.wait_recv()
    for c in range(PROJ_CHUNKS):
        near_copy(c).wait_recv()
    def hidden_of(y, scaled_ref, acc_ref, residual_of):
        squares = jnp.sum(y * y, axis=1, keepdims=True)
        scaled_ref[...] = (y * gain_ref[...]).astype(bf16)
        scale = lax.rsqrt(squares / total_chans + 1e-06)

        def project(cols):
            weights = proj_all[:, :, cols].reshape(total_chans, 256)
            part = dot(scaled_ref[...], weights)
            acc_ref[:, cols] = deep_alpha * residual_of(cols).astype(f32) + part * scale

        every(width, 256, project)
        return layer_norm(acc_ref[...], mix_gain_ref[...]).astype(bf16)

    def back_copy(peer, source, columns=None):
        cols = pl.ds(0, columns or width)
        return pltpu.make_async_remote_copy(
            ret_out.at[peer, :, cols], ret_in.at[source, :, cols],
            back_s.at[peer], back_r.at[source], device_id={"sp": peer},
        )

    def far_back(body):
        for t in order:
            for column in range(LO):
                body(apart + LO * t + column)

    def expert(sources, way=None):
        count = len(sources) * cap
        for source in sources:
            @pl.when(source != sp)
            def _():
                y_copy(source, source).wait_recv()
        top = pl.ds(0, count)
        y = jnp.concatenate([y_in[source] for source in sources], axis=0).astype(f32)
        hid_b[top, :] = hidden_of(
            y, scaled_v.at[top], acc_b.at[top],
            lambda cols: jnp.concatenate([res_in[source, :, cols] for source in sources], axis=0),
        )
        rows_b = hid_b[top, :]
        gate, up = dot(rows_b, gate_v[...]), dot(rows_b, up_v[...])
        active = (gate * jax.nn.sigmoid(gate) * up).astype(bf16)

        def produce(cols):
            made = dot(active, down_v[:, cols]).astype(bf16)
            for j, source in enumerate(sources):
                ret_out[source, :, cols] = made[j * cap : (j + 1) * cap]

        every(width, 256, produce)
        if way is None:
            for source in sources:
                @pl.when(source != sp)
                def _():
                    back_copy(source, sp).start()
            return
        column = lo if way == 0 else 1 - lo
        for t, source in zip(order, sources):
            if way == 0:
                @pl.when(is_gate)
                def _():
                    gate_in[t, sp - close] = ret_out[source, :, pl.ds(keep, width - keep)]

                @pl.when(~is_gate)
                def _():
                    part_copy(t, column, way).start()
            else:
                part_copy(t, column, way).start()
        for source in sources:
            back_copy(source, sp, keep).start()

    def sum_ready(t):
        for c in range(take):
            @pl.when(c != sp - close)
            def _():
                part_arrived(t, c)
        pltpu.make_async_remote_copy(
            gate_w.at[t], gate_w.at[t], gw_s.at[0], gw_r.at[t], device_id={"sp": mate * LO + lo},
        ).wait_recv()
        got = gate_in[t].reshape(BATCH_ROWS, width - keep)
        whole = dot(gate_w[t, 0], got, TN) + dot(gate_w[t, 1], got, TN)
        gate_out[t] = whole.astype(bf16)
        sum_copy(t).start()

    if flood:
        for copy in loads[1:]:
            copy.wait()
        their_weight().start()
        expert([apart + LO * t + lo for t in order], 0)
        for owner in beyond:
            res_copy(owner).wait_recv()
        expert([apart + LO * t + 1 - lo for t in order], 1)
        for owner in (hi, mate):
            res_copy(owner).wait_recv()
        expert([close + j for j in range(take)])
    else:
        repeat(n_sp - 1, lambda k: send_res(k).wait_recv())
        for copy in loads[1:]:
            copy.wait()
        repeat(batches, lambda i: expert([batch_of(i) * take + j for j in range(take)]))
    ret_in[sp] = ret_out[sp]
    y = jnp.concatenate([mix_in[part].astype(f32) for part in range(n_tp)], axis=1)
    hid[...] = hidden_of(y, scaled_v.at[pl.ds(0, rows)], acc, lambda cols: res_ref[:, cols])
    if flood:
        @pl.when(is_gate)
        def _():
            for t in order:
                sum_ready(t)

        others(0, lambda peer: back_copy(peer, peer).wait_recv())
        far_back(lambda peer: back_copy(peer, peer, keep).wait_recv())
        sum_copy(0).wait_recv()
    else:
        repeat(batches, lambda i: others(i, lambda peer: back_copy(peer, peer).wait_recv()))

    def combine(cols):
        got = ret_in[:, :, cols].reshape(slots, 256)
        acc[:, cols] = (
            deep_alpha * hid[:, cols].astype(f32) + dot(w_high, got, TN) + dot(w_low, got, TN)
        )

    def combine_close(cols):
        got = ret_in[pl.ds(close, take), :, pl.ds(cols.start + keep, cols.size)]
        got = got.reshape(BATCH_ROWS, cols.size)
        slab = pl.ds(pl.multiple_of(close * cap, BATCH_ROWS), BATCH_ROWS)
        there = pl.ds(cols.start + keep, cols.size)
        acc[:, there] = (
            deep_alpha * hid[:, there].astype(f32) + sum_in[:, cols].astype(f32)
            + dot(w_out[0, slab, :], got, TN) + dot(w_out[1, slab, :], got, TN)
        )

    every(keep, 256, combine)
    if flood:
        every(width - keep, 256, combine_close)
    o_ref[...] = layer_norm(acc[...], final_gain_ref[...]).astype(bf16)

    for c in sent:
        far_copy(c).wait_send()
    for c in relayed:
        relay_copy(c).wait_send()
    for c in range(PROJ_CHUNKS):
        near_copy(c).wait_send()
    for copy in [proj_near] + mixes:
        copy.wait_send()
    repeat(n_sp - 1, carry_sent)
    if flood:
        repeat(line - 1, lambda k: pick_copy(k).wait_send())
        for part in range(PIECES):
            for kind in range(2):
                raw_copy(kind, part).wait_send()

        @pl.when(is_gate)
        def _():
            for part in range(PIECES):
                for i in range(2):
                    via_copy(i, part).wait_send()

        for owner in range(line):
            res_copy(owner).wait_send()
    else:
        repeat(n_sp - 1, lambda k: send_res(k).wait_send())
    repeat(batches, lambda i: others(i, lambda peer: y_copy(peer, sp).wait_send()))
    if flood:
        others(0, lambda peer: back_copy(peer, sp).wait_send())
        far_back(lambda peer: back_copy(peer, sp, keep).wait_send())
        their_weight().wait_send()
        for t in range(2):
            @pl.when(~is_gate)
            def _():
                part_copy(t, lo, 0).wait_send()

            part_copy(t, 1 - lo, 1).wait_send()

            @pl.when(is_gate)
            def _():
                sum_copy(t).wait_send()
    else:
        repeat(batches, lambda i: others(i, lambda peer: back_copy(peer, sp).wait_send()))


def local(
    mixer_input, retention, decay_real, decay_freq, log_step, input_real, input_imag,
    readout_real, readout_imaginary, skip_weight, norm_gain, projection, residual, mix_gain,
    routes, route_weight, expert_gate, expert_up, expert_down, final_gain,
):
    n_sp, n_tp = lax.axis_size("sp"), lax.axis_size("tp")
    tokens, chans = mixer_input.shape
    groups, states, channels = input_real.shape
    gp, rows, width = groups * states, residual.shape[0], residual.shape[1]
    cap = -(-max(2, 2 * rows * PICKS // n_sp) // 16) * 16
    hidden, line = expert_gate.shape[2], n_sp // LO
    take = BATCH_ROWS // cap
    rest = width - width // DIRECT_SHARE if n_sp == 8 else 128

    def compact(value):
        return jnp.swapaxes(value, 1, 2).reshape(chans, states)

    small = (
        mixer_input, retention, decay_real, decay_freq, log_step[None, :], skip_weight,
        norm_gain[None, :], compact(input_real), compact(input_imag),
        readout_real.reshape(chans, states), readout_imaginary.reshape(chans, states),
        residual, mix_gain[None, :], routes.T, route_weight.T, final_gain[None, :],
    )
    vmem = pl.BlockSpec(memory_space=pltpu.VMEM)
    anywhere = pl.BlockSpec(memory_space=pl.ANY)
    dma = pltpu.SemaphoreType.DMA
    return pl.pallas_call(
        functools.partial(kernel, n_sp, n_tp, groups, channels, states, cap),
        out_shape=jax.ShapeDtypeStruct((rows, width), bf16),
        in_specs=[anywhere] * (len(small) + 4),
        out_specs=vmem,
        scratch_shapes=[pltpu.VMEM(value.shape, value.dtype) for value in small]
        + [
            pltpu.VMEM((tokens, gp), f32),
            pltpu.VMEM((tokens, gp), f32),
            pltpu.VMEM((tokens, gp), f32),
            pltpu.VMEM((3, gp), f32),
            pltpu.VMEM((n_sp, 3, gp), f32),
            pltpu.VMEM((tokens, chans), bf16),
            pltpu.VMEM((n_tp, rows, chans), bf16),
            pltpu.VMEM((n_tp,) + projection.shape, bf16),
            pltpu.VMEM((width, hidden), bf16),
            pltpu.VMEM((width, hidden), bf16),
            pltpu.VMEM((hidden, width), bf16),
            pltpu.VMEM((rows, width), f32),
            pltpu.VMEM((rows, width), bf16),
            pltpu.VMEM((BATCH_ROWS, n_tp * chans), bf16),
            pltpu.VMEM((BATCH_ROWS, width), f32),
            pltpu.VMEM((BATCH_ROWS, width), bf16),
            pltpu.VMEM((n_sp * cap, rows), bf16),
            pltpu.VMEM((line, LO * cap, rows), bf16),
            pltpu.VMEM((line, rows, width) if n_sp == 8 else (1, 16, 128), bf16),
            pltpu.VMEM((n_sp, cap, width), bf16),
            pltpu.VMEM((n_sp, cap, width), bf16),
            pltpu.VMEM((n_sp, cap, n_tp * chans), bf16),
            pltpu.VMEM((n_sp, cap, n_tp * chans), bf16),
            pltpu.VMEM((n_sp, cap, width), bf16),
            pltpu.VMEM((n_sp, cap, width), bf16),
            pltpu.VMEM((2, n_sp * cap, rows), bf16),
            pltpu.VMEM((2, 2, take * cap, rows), bf16),
            pltpu.VMEM((2, take, cap, rest), bf16),
            pltpu.VMEM((2, rows, rest), bf16),
            pltpu.VMEM((rows, rest), bf16),
            dma((len(small),)), dma((4,)),
            dma((n_sp,)), dma((n_sp,)),
            dma((n_tp,)), dma((n_tp,)),
            dma((PROJ_CHUNKS + 1,)), dma((PROJ_CHUNKS + 1,)),
            dma((PROJ_CHUNKS,)), dma((PROJ_CHUNKS,)),
            dma((PROJ_CHUNKS,)), dma((line,)), dma((line,)),
            dma((2 * PIECES,)), dma((line * PIECES,)), dma((2 * PIECES,)),
            dma((n_sp,)), dma((n_sp,)),
            dma((n_sp,)), dma((n_sp,)),
            dma((n_sp,)), dma((n_sp,)),
            dma((1,)), dma((2,)), dma((4,)), dma((2 * take,)), dma((2,)), dma((1,)),
        ],
        compiler_params=pltpu.CompilerParams(
            collective_id=0, has_side_effects=True, vmem_limit_bytes=60 * 1024 * 1024
        ),
    )(
        *small,
        projection, expert_gate, expert_up, expert_down,
    )


def solution(mesh):
    in_specs = (
        P("sp", "tp"),
        P("tp", "sp"),
        P("tp", None),
        P("tp", None),
        P("tp"),
        P("tp", None, None),
        P("tp", None, None),
        P("tp", None, None),
        P("tp", None, None),
        P("tp", None),
        P(),
        P("tp", None),
        P(("sp", "tp"), None),
        P(),
        P(("sp", "tp"), None),
        P(("sp", "tp"), None),
        P("sp", None, None),
        P("sp", None, None),
        P("sp", None, None),
        P(),
    )
    out_specs = P(("sp", "tp"), None)
    return jax.shard_map(local, mesh=mesh, in_specs=in_specs, out_specs=out_specs, check_vma=False)
```

```python
import functools

import jax
import jax.numpy as jnp
from jax import lax
from jax.experimental import pallas as pl
from jax.experimental.pallas import tpu as pltpu
from jax.sharding import PartitionSpec as P

PICKS = 2
SPANS = 8
deep_alpha = 2.0**0.25
f32, bf16 = jnp.float32, jnp.bfloat16
highest = lax.Precision.HIGHEST
NT = (((1,), (1,)), ((), ()))
TN = (((0,), (0,)), ((), ()))
PROJ_CHUNKS = 8
PROJ_RELAY = 1
PROJ_FIRST = 1
PROJ_NEXT = 2
EARLY = 2
DIRECT_SHARE = 2
LO = 2
PIECES = 4
BATCH_ROWS = 128


def dot(a, b, dims=None, precision=None):
    dims = dims or (((1,), (0,)), ((), ()))
    return lax.dot_general(a, b, dims, precision=precision, preferred_element_type=f32)


def split(value):
    high = value.astype(bf16)
    return high, (value - high.astype(f32)).astype(bf16)


def iota(shape, dim):
    return lax.broadcasted_iota(jnp.int32, shape, dim)


def layer_norm(values, scales):
    centered = values - jnp.mean(values, axis=-1, keepdims=True)
    variance = jnp.mean(centered * centered, axis=-1, keepdims=True)
    return centered * lax.rsqrt(variance + 1e-05) * scales


def cmul(ar, ai, br, bi):
    return ar * br - ai * bi, ar * bi + ai * br


def expm1(value, grown):
    series = value * 0.125 + 1.0
    for k in range(7, 1, -1):
        series = series * value * (1.0 / k) + 1.0
    return jnp.where(value > -0.4, series * value, grown - 1.0)


def repeat(count, body):
    if count <= 8:
        for k in range(count):
            body(k)
    else:
        lax.fori_loop(0, count, lambda k, c: (body(k), c)[1], 0)


def kernel(
    n_sp, n_tp, groups, channels, states, cap,
    x_hbm, ret_hbm, real_hbm, freq_hbm, step_hbm, skip_hbm, gain_hbm, in_re_hbm, in_im_hbm,
    out_re_hbm, out_im_hbm, res_hbm, mix_gain_hbm, routes_hbm, rw_hbm, final_gain_hbm,
    proj_ref, gate_ref, up_ref, down_ref,
    o_ref,
    x_ref, ret_ref, real_ref, freq_ref, step_ref, skip_ref, gain_ref, in_re_ref, in_im_ref,
    out_re_ref, out_im_ref, res_ref, mix_gain_ref, routes_ref, rw_ref, final_gain_ref,
    d_re, d_im, shr, carry_out, carry_in, mix_out, mix_in, proj_all, gate_v, up_v, down_v,
    acc, hid, scaled_v, acc_b, hid_b, pick_out, pick_in, raw, res_out, res_in, y_out, y_in,
    ret_out, ret_in, w_out, gate_w, gate_in, gate_out, sum_in,
    in_sem, w_sem, car_s, car_r, mix_s, mix_r, prj_s, prj_r, fwd_s, fwd_r,
    rel_s, pick_s, pick_r, raw_s, raw_r, via_s, res_s, res_r, y_s, y_r, back_s, back_r, gw_s, gw_r, gc_s, gc_r, sum_s, sum_r,
):
    sp, tp = lax.axis_index("sp"), lax.axis_index("tp")
    tokens, chans = x_ref.shape
    gp = groups * states
    span = tokens // SPANS
    rows = tokens // n_tp
    width = o_ref.shape[1]

    small = (
        (step_hbm, step_ref), (real_hbm, real_ref), (freq_hbm, freq_ref), (in_re_hbm, in_re_ref),
        (in_im_hbm, in_im_ref), (x_hbm, x_ref), (ret_hbm, ret_ref), (skip_hbm, skip_ref),
        (out_re_hbm, out_re_ref), (out_im_hbm, out_im_ref), (gain_hbm, gain_ref),
        (routes_hbm, routes_ref), (rw_hbm, rw_ref), (res_hbm, res_ref),
        (mix_gain_hbm, mix_gain_ref), (final_gain_hbm, final_gain_ref),
    )
    fetches = [
        pltpu.make_async_copy(src, dst, in_sem.at[i]) for i, (src, dst) in enumerate(small)
    ]
    for fetch in fetches:
        fetch.start()

    barrier = pltpu.get_barrier_semaphore()

    def greet_sp(k):
        pl.semaphore_signal(barrier, inc=1, device_id={"sp": lax.rem(sp + k + 1, n_sp)})

    def greet_tp(k):
        pl.semaphore_signal(barrier, inc=1, device_id={"tp": lax.rem(tp + k + 1, n_tp)})

    repeat(n_sp - 1, greet_sp)
    repeat(n_tp - 1, greet_tp)

    own = pltpu.make_async_copy(proj_ref, proj_all.at[tp], w_sem.at[0])
    own.start()
    loads = [own]
    for i, (src, dst) in enumerate(((gate_ref, gate_v), (up_ref, up_v), (down_ref, down_v))):
        loads.append(pltpu.make_async_copy(src.at[0], dst, w_sem.at[i + 1]))
        loads[-1].start()
    pl.semaphore_wait(barrier, n_sp - 1 + n_tp - 1)

    depth = proj_ref.shape[0] // PROJ_CHUNKS
    near = tp + 1 - 2 * lax.rem(tp, 2)
    far = lax.rem(tp + 2, n_tp)
    hi, lo = sp // LO, lax.rem(sp, LO)
    line = n_sp // LO
    flood = n_sp == 8

    def piece(i):
        return pl.ds(i * depth, depth)

    direct = PROJ_CHUNKS - LO * PROJ_RELAY
    relayed = [direct + PROJ_RELAY * lo + i for i in range(PROJ_RELAY)]
    foreign = [direct + PROJ_RELAY * (1 - lo) + i for i in range(PROJ_RELAY)]
    sent = relayed + list(range(direct))

    def far_copy(c):
        return pltpu.make_async_remote_copy(
            proj_ref.at[piece(c)], proj_all.at[tp, piece(c)], prj_s.at[c], prj_r.at[c],
            device_id={"tp": far},
        )

    def far_chunk(c):
        return proj_all.at[far, piece(c)]

    def relay_copy(c):
        return pltpu.make_async_remote_copy(
            far_chunk(c), far_chunk(c), rel_s.at[c], prj_r.at[c],
            device_id={"sp": hi * LO + 1 - lo},
        )

    def near_copy(c):
        return pltpu.make_async_remote_copy(
            far_chunk(c), far_chunk(c), fwd_s.at[c], fwd_r.at[c], device_id={"tp": near},
        )

    proj_near = pltpu.make_async_remote_copy(
        proj_ref, proj_all.at[tp], prj_s.at[PROJ_CHUNKS], prj_r.at[PROJ_CHUNKS],
        device_id={"tp": near},
    )
    for c in sent[: PROJ_RELAY + PROJ_FIRST]:
        far_copy(c).start()
    following = sent[PROJ_RELAY + PROJ_FIRST : PROJ_RELAY + PROJ_FIRST + PROJ_NEXT]

    @pl.when(hi >= line // 2)
    def _():
        for c in following:
            far_copy(c).start()


    for fetch in fetches:
        fetch.wait()

    slots = n_sp * cap
    expert_of = iota((slots, rows), 0) // cap
    hit0 = routes_ref[0:1, :] == expert_of
    hit1 = routes_ref[1:2, :] == expert_of
    member = jnp.where(hit0 | hit1, 1.0, 0.0)
    upper = jnp.where(iota((rows, rows), 0) < iota((rows, rows), 1), 1.0, 0.0).astype(bf16)
    place = dot(member.astype(bf16), upper)
    wanted = lax.rem(iota((slots, rows), 0), cap).astype(f32)
    chosen = jnp.where(place == wanted, member, 0.0)
    weight = chosen * jnp.where(hit0, rw_ref[0:1, :], rw_ref[1:2, :])
    chosen = chosen.astype(bf16)
    w_high, w_low = split(weight)

    def every(count, width, body):
        if flood:
            for i in range(count // width):
                body(pl.ds(i * width, width))
            return

        def step(i, c):
            body(pl.ds(pl.multiple_of(i * width, width), width))
            return c

        lax.fori_loop(0, count // width, step, 0)

    piece_rows = rows // PIECES
    mate = hi + 1 - 2 * lax.rem(hi, 2)
    gate_node = 2 - hi // 2
    is_gate = (hi == 1) | (hi == 2)
    beyond = [gate_node, 3 * (1 - hi // 2)]

    def pick_copy(k):
        peer = lax.rem(hi + k + 1, line)
        return pltpu.make_async_remote_copy(
            pick_out.at[pl.ds(pl.multiple_of(peer * LO * cap, LO * cap), LO * cap)],
            pick_in.at[hi], pick_s.at[k], pick_r.at[k], device_id={"sp": peer * LO + lo},
        )

    def rows_at(part):
        return pl.ds(part * piece_rows, piece_rows)

    def raw_copy(kind, part):
        return pltpu.make_async_remote_copy(
            res_ref.at[rows_at(part)], raw.at[hi, rows_at(part)],
            raw_s.at[kind * PIECES + part], raw_r.at[hi * PIECES + part],
            device_id={"sp": (gate_node if kind == 0 else mate) * LO + lo},
        )

    def via_copy(i, part):
        owner = beyond[i]
        return pltpu.make_async_remote_copy(
            raw.at[owner, rows_at(part)], raw.at[owner, rows_at(part)],
            via_s.at[i * PIECES + part], raw_r.at[owner * PIECES + part],
            device_id={"sp": mate * LO + lo},
        )

    def raw_start(kind, part, upward):
        node = mate if kind else gate_node

        @pl.when(node > hi if upward else node < hi)
        def _():
            raw_copy(kind, part).start()

    def raw_arrived(owner, part):
        pltpu.make_async_remote_copy(
            raw.at[owner, rows_at(part)], raw.at[owner, rows_at(part)],
            raw_s.at[part], raw_r.at[owner * PIECES + part], device_id={"sp": mate * LO + lo},
        ).wait_recv()

    def forward(i, part):
        @pl.when(is_gate)
        def _():
            raw_arrived(beyond[i], part)
            via_copy(i, part).start()

    def res_copy(owner):
        return pltpu.make_async_remote_copy(
            res_out.at[owner * LO + 1 - lo], res_in.at[owner * LO + lo],
            res_s.at[owner], res_r.at[owner], device_id={"sp": hi * LO + 1 - lo},
        )

    def share(owner, pick, rows_of):
        def step(cols):
            both = dot(pick, rows_of[:, cols]).astype(bf16).reshape(LO, cap, 256)
            res_out[pl.ds(owner * LO, LO), :, cols] = both

        every(width, 256, step)
        res_in[owner * LO + lo] = res_out[owner * LO + lo]
        res_copy(owner).start()

    def share_line(owner):
        share(owner, pick_in[owner], raw.at[owner])

    def send_res(k):
        peer = lax.rem(sp + k + 1, n_sp)
        return pltpu.make_async_remote_copy(
            res_out.at[peer], res_in.at[sp], res_s.at[k], res_r.at[k], device_id={"sp": peer}
        )

    take = BATCH_ROWS // cap
    batches = n_sp // take
    home = sp // take

    def batch_of(i):
        return lax.rem(home + i, batches) if batches > 1 else 0

    close, apart = home * take, batch_of(1) * take
    keep = width // DIRECT_SHARE if flood else width
    turn = hi // 2
    order = (1 - turn, turn)

    def their_weight():
        slab = pl.ds(pl.multiple_of(apart * cap, BATCH_ROWS), BATCH_ROWS)
        return pltpu.make_async_remote_copy(
            w_out.at[:, slab], gate_w.at[lax.rem(hi, 2)], gw_s.at[0], gw_r.at[lax.rem(hi, 2)],
            device_id={"sp": gate_node * LO + lo},
        )

    def part_copy(t, column, way):
        return pltpu.make_async_remote_copy(
            ret_out.at[apart + LO * t + column, :, pl.ds(keep, width - keep)],
            gate_in.at[t, sp - close], gc_s.at[2 * way + t], gc_r.at[t * take + sp - close],
            device_id={"sp": (1 + turn) * LO + column},
        )

    def part_arrived(t, c):
        pltpu.make_async_remote_copy(
            gate_in.at[t, c], gate_in.at[t, c], gc_s.at[0], gc_r.at[t * take + c],
            device_id={"sp": mate * LO + lo},
        ).wait_recv()

    def sum_copy(t):
        return pltpu.make_async_remote_copy(
            gate_out.at[t], sum_in, sum_s.at[t], sum_r.at[0],
            device_id={"sp": apart + LO * t + lo},
        )

    pick_out[...] = chosen
    w_out[0] = w_high
    w_out[1] = w_low
    if flood:
        repeat(line - 1, lambda k: pick_copy(k).start())
        for kind in (1, 0):
            for part in range(PIECES):
                raw_start(kind, part, False)

        @pl.when(hi > 0)
        def _():
            for part in range(3):
                raw_start(0, part, True)

        for part in range(EARLY):
            raw_start(1, part, True)
        share(hi, pick_out[pl.ds(pl.multiple_of(hi * LO * cap, LO * cap), LO * cap), :], res_ref)
    else:
        def spread_res(cols):
            res_out[:, :, cols] = dot(chosen, res_ref[:, cols]).astype(bf16).reshape(n_sp, cap, 256)

        every(width, 256, spread_res)
        res_in[sp] = res_out[sp]
        repeat(n_sp - 1, lambda k: send_res(k).start())

    eye = iota((groups, groups), 0) == iota((groups, groups), 1)
    stride = jnp.exp(jnp.sum(jnp.where(eye, step_ref[...], 0.0), axis=1, keepdims=True))
    real, freq = real_ref[...], freq_ref[...]
    growth, turning = real * stride, freq * stride
    cosine, sine, half = jnp.cos(turning), jnp.sin(turning), jnp.sin(0.5 * turning)
    size = jnp.exp(growth)
    upper_real = expm1(growth, size) * cosine - 2.0 * half * half
    keep_re, upper_imag = size * cosine, size * sine
    denominator = real * real + freq * freq
    f_re = (upper_real * real + upper_imag * freq) / denominator
    f_im = (upper_imag * real - upper_real * freq) / denominator
    big_re, big_im = keep_re, upper_imag
    for _ in range(span.bit_length() - 1):
        big_re, big_im = cmul(big_re, big_im, big_re, big_im)
    full_re, full_im = big_re, big_im
    for _ in range(SPANS.bit_length() - 1):
        full_re, full_im = cmul(full_re, full_im, full_re, full_im)

    tile_p = jnp.where(
        lax.rem(iota((states, gp), 1), states) == iota((states, gp), 0), 1.0, 0.0
    )
    widen = jnp.where(
        iota((groups, gp), 1) // states == iota((groups, gp), 0), 1.0, 0.0
    ).astype(f32)
    packed = jnp.concatenate([keep_re, upper_imag, big_re, big_im, full_re, full_im], axis=0)
    spread = dot(packed, tile_p, precision=highest)
    k_re, k_im, b_re, b_im, full_re, full_im = [
        jnp.sum(spread[i * groups : (i + 1) * groups] * widen, axis=0, keepdims=True)
        for i in range(6)
    ]
    tile_p = tile_p.astype(bf16)
    mask_out = iota((chans, gp), 0) // channels == iota((chans, gp), 1) // states

    def wide(value):
        return [
            jnp.where(mask_out, dot(part, tile_p), 0.0).astype(bf16) for part in split(value)
        ]

    copies = jnp.where(
        iota((chans, groups), 0) // channels == iota((chans, groups), 1), 1.0, 0.0
    ).astype(f32)
    f_re, f_im = dot(copies, f_re, precision=highest), dot(copies, f_im, precision=highest)
    bar_re, bar_im = cmul(f_re, f_im, in_re_ref[...], in_im_ref[...])

    row_i, col_i = iota((tokens, tokens), 0), iota((tokens, tokens), 1)
    perm = jnp.where(
        col_i == lax.rem(row_i, SPANS) * span + row_i // SPANS, 1.0, 0.0
    ).astype(bf16)
    x = dot(perm, x_ref[...]).astype(bf16)
    for bar, d_ref in ((bar_re, d_re), (bar_im, d_im)):
        high, low = wide(bar)
        d_ref[...] = dot(x, high) + dot(x, low)
    held = jnp.exp(ret_ref[...])
    first_part = held.astype(bf16)
    rest = held - first_part.astype(f32)
    held = dot(jnp.concatenate([first_part, *split(rest)], axis=0), perm, NT).astype(bf16)
    shr[...] = dot(held, jnp.concatenate([widen.astype(bf16)] * 3, axis=0), TN)

    k_re = jnp.broadcast_to(k_re, (SPANS, gp))
    k_im = jnp.broadcast_to(k_im, (SPANS, gp))

    def advance(j, s_re, s_im):
        at = pl.ds(pl.multiple_of(j * SPANS, SPANS), SPANS)
        m_re, m_im = cmul(k_re, k_im, s_re, s_im)
        shrink = shr[at, :]
        return at, shrink, shrink * m_re + d_re[at, :], shrink * m_im + d_im[at, :]

    def first(j, state):
        s_re, s_im, total = state
        _, shrink, s_re, s_im = advance(j, s_re, s_im)
        return s_re, s_im, total * shrink

    zero = jnp.zeros((SPANS, gp), f32)
    e_re, e_im, total = lax.fori_loop(0, span, first, (zero, zero, zero + 1.0))
    a_re, a_im = total * b_re, total * b_im

    one = jnp.ones((1, gp), f32)
    nil = jnp.zeros((1, gp), f32)
    c_re, c_im, s_re, s_im = one, nil, nil, nil
    entries = []
    for i in range(SPANS):
        entries.append((c_re, c_im, s_re, s_im))
        ar, ai = a_re[i : i + 1], a_im[i : i + 1]
        s_re, s_im = cmul(ar, ai, s_re, s_im)
        s_re, s_im = s_re + e_re[i : i + 1], s_im + e_im[i : i + 1]
        c_re, c_im = cmul(ar, ai, c_re, c_im)
    held_all = total[0:1]
    for i in range(1, SPANS):
        held_all = held_all * total[i : i + 1]
    for i, part in enumerate((held_all, s_re, s_im)):
        carry_out[i : i + 1, :] = part

    def carry_copy(k):
        return pltpu.make_async_remote_copy(
            carry_out, carry_in.at[sp], car_s.at[k], car_r.at[k],
            device_id={"sp": lax.rem(sp + k + 1, n_sp)},
        )

    def carry_start(k):
        @pl.when(sp + k + 1 < n_sp)
        def _():
            carry_copy(k).start()

    def carry_arrived(k):
        @pl.when(sp > k)
        def _():
            carry_copy(k).wait_recv()

    def carry_sent(k):
        @pl.when(sp + k + 1 < n_sp)
        def _():
            carry_copy(k).wait_send()

    repeat(n_sp - 1, lambda k: carry_start(n_sp - 2 - k))
    if flood:
        for part in range(EARLY, PIECES):
            raw_start(1, part, True)

        @pl.when(hi > 0)
        def _():
            for part in range(3, PIECES):
                raw_start(0, part, True)

        forward(0, 0)
    c_re, c_im, s_re, s_im = [
        jnp.concatenate([entry[i] for entry in entries], axis=0) for i in range(4)
    ]

    o_re, o_im = wide(out_re_ref[...]), wide(out_im_ref[...])
    tile_c = jnp.where(
        lax.rem(iota((channels, chans), 1), channels) == iota((channels, chans), 0), 1.0, 0.0
    ).astype(f32)
    own_group = iota((groups, chans), 1) // channels == iota((groups, chans), 0)
    skip = jnp.where(own_group, dot(skip_ref[...], tile_c, precision=highest), 0.0)
    skip = jnp.sum(skip, axis=0, keepdims=True)

    if flood:
        forward(0, 1)
    repeat(n_sp - 1, carry_arrived)
    if flood:
        forward(0, 2)
    for c in relayed:
        far_copy(c).wait_recv()
        relay_copy(c).start()
        near_copy(c).start()

    def fold(position, state):
        part = carry_in[position]
        n_re, n_im = cmul(part[0:1] * full_re, part[0:1] * full_im, *state)
        return (
            jnp.where(position < sp, n_re + part[1:2], state[0]),
            jnp.where(position < sp, n_im + part[2:3], state[1]),
        )

    state = (nil, nil)
    if n_sp <= 8:
        for position in range(n_sp - 1):
            state = fold(position, state)
    else:
        state = lax.fori_loop(0, n_sp - 1, fold, state)
    m_re, m_im = cmul(c_re, c_im, *state)

    def second(j, state):
        at, _, s_re, s_im = advance(j, *state)
        d_re[at, :] = s_re
        d_im[at, :] = s_im
        return s_re, s_im

    lax.fori_loop(0, span, second, (s_re + m_re, s_im + m_im))

    def read(ref, wide):
        high, low = split(ref[...])
        return dot(high, wide[0], NT) + dot(low, wide[0], NT) + dot(high, wide[1], NT)

    y = read(d_re, o_re) - read(d_im, o_im) + skip * x.astype(f32)
    y = jax.nn.gelu(y).astype(bf16)
    mix_out[...] = dot(perm, y, TN).astype(bf16)

    def mine(index):
        return pl.ds(pl.multiple_of(index * rows, rows), rows)

    mixes = []
    for k in range(n_tp - 1):
        peer = lax.rem(tp + k + 1, n_tp)
        mixes.append(
            pltpu.make_async_remote_copy(
                mix_out.at[mine(peer)], mix_in.at[tp], mix_s.at[k], mix_r.at[k],
                device_id={"tp": peer},
            )
        )
        mixes[-1].start()

    @pl.when(hi < line // 2)
    def _():
        for c in following:
            far_copy(c).start()

    for c in sent[PROJ_RELAY + PROJ_FIRST + PROJ_NEXT :]:
        far_copy(c).start()
    proj_near.start()
    mix_in[tp] = mix_out[mine(tp), :]
    if flood:
        @pl.when(hi == 0)
        def _():
            for part in range(PIECES):
                raw_copy(0, part).start()

    if flood:
        forward(0, 3)
        forward(1, 0)
        repeat(line - 1, lambda k: pick_copy(k).wait_recv())
        for part in range(PIECES):
            raw_arrived(mate, part)
        share_line(mate)
        forward(1, 1)
    for copy in mixes:
        copy.wait_recv()
    if flood:
        @pl.when(hi == 0)
        def _():
            for part in range(PIECES):
                raw_arrived(beyond[0], part)

    total_chans = n_tp * chans
    for part in range(n_tp):
        y_out[:, :, part * chans : (part + 1) * chans] = (
            dot(chosen, mix_in[part]).astype(bf16).reshape(n_sp, cap, chans)
        )

    def others(i, body, backward=False):
        base = batch_of(i) * take

        def one(j):
            peer = base + (take - 1 - j if backward else j)

            @pl.when(peer != sp)
            def _():
                body(peer)

        repeat(take, one)

    def y_copy(peer, source):
        return pltpu.make_async_remote_copy(
            y_out.at[peer], y_in.at[source], y_s.at[peer], y_r.at[source], device_id={"sp": peer}
        )

    def y_start(i):
        outward = home < batches // 2

        @pl.when(outward)
        def _():
            others(i, lambda peer: y_copy(peer, sp).start(), True)

        @pl.when(~outward)
        def _():
            others(i, lambda peer: y_copy(peer, sp).start())

    if flood:
        forward(1, 2)
        forward(1, 3)
    repeat(batches, lambda i: y_start(batches - 1 - i))
    y_in[sp] = y_out[sp]

    def project_arrived(chunks):
        for c in chunks:
            far_copy(c).wait_recv()
            near_copy(c).start()

    def far_share(i):
        @pl.when(~is_gate & ((hi > 0) | (i > 0)))
        def _():
            for part in range(PIECES):
                raw_arrived(beyond[i], part)

        share_line(beyond[i])

    if flood:
        far_share(0)

        @pl.when(is_gate)
        def _():
            far_share(1)

        project_arrived(list(range(direct)) + foreign)

        @pl.when(~is_gate)
        def _():
            far_share(1)

    else:
        project_arrived(list(range(direct)) + foreign)
    own.wait()
    proj_near.wait_recv()
    for c in range(PROJ_CHUNKS):
        near_copy(c).wait_recv()
    def hidden_of(y, scaled_ref, acc_ref, residual_of):
        squares = jnp.sum(y * y, axis=1, keepdims=True)
        scaled_ref[...] = (y * gain_ref[...]).astype(bf16)
        scale = lax.rsqrt(squares / total_chans + 1e-06)

        def project(cols):
            weights = proj_all[:, :, cols].reshape(total_chans, 256)
            part = dot(scaled_ref[...], weights)
            acc_ref[:, cols] = deep_alpha * residual_of(cols).astype(f32) + part * scale

        every(width, 256, project)
        return layer_norm(acc_ref[...], mix_gain_ref[...]).astype(bf16)

    def back_copy(peer, source, columns=None):
        cols = pl.ds(0, columns or width)
        return pltpu.make_async_remote_copy(
            ret_out.at[peer, :, cols], ret_in.at[source, :, cols],
            back_s.at[peer], back_r.at[source], device_id={"sp": peer},
        )

    def far_back(body):
        for t in order:
            for column in range(LO):
                body(apart + LO * t + column)

    def expert(sources, way=None):
        count = len(sources) * cap
        for source in sources:
            @pl.when(source != sp)
            def _():
                y_copy(source, source).wait_recv()
        top = pl.ds(0, count)
        y = jnp.concatenate([y_in[source] for source in sources], axis=0).astype(f32)
        hid_b[top, :] = hidden_of(
            y, scaled_v.at[top], acc_b.at[top],
            lambda cols: jnp.concatenate([res_in[source, :, cols] for source in sources], axis=0),
        )
        rows_b = hid_b[top, :]
        gate, up = dot(rows_b, gate_v[...]), dot(rows_b, up_v[...])
        active = (gate * jax.nn.sigmoid(gate) * up).astype(bf16)

        def produce(cols):
            made = dot(active, down_v[:, cols]).astype(bf16)
            for j, source in enumerate(sources):
                ret_out[source, :, cols] = made[j * cap : (j + 1) * cap]

        every(width, 256, produce)
        if way is None:
            for source in sources:
                @pl.when(source != sp)
                def _():
                    back_copy(source, sp).start()
            return
        column = lo if way == 0 else 1 - lo
        for t, source in zip(order, sources):
            if way == 0:
                @pl.when(is_gate)
                def _():
                    gate_in[t, sp - close] = ret_out[source, :, pl.ds(keep, width - keep)]

                @pl.when(~is_gate)
                def _():
                    part_copy(t, column, way).start()
            else:
                part_copy(t, column, way).start()
        if way == 0:
            @pl.when(is_gate)
            def _():
                for source in sources:
                    back_copy(source, sp, keep).start()
        else:
            @pl.when(~is_gate)
            def _():
                for t in order:
                    back_copy(apart + LO * t + lo, sp, keep).start()

            for source in sources:
                back_copy(source, sp, keep).start()

    def sum_ready(t):
        for c in range(take):
            @pl.when(c != sp - close)
            def _():
                part_arrived(t, c)
        pltpu.make_async_remote_copy(
            gate_w.at[t], gate_w.at[t], gw_s.at[0], gw_r.at[t], device_id={"sp": mate * LO + lo},
        ).wait_recv()
        got = gate_in[t].reshape(BATCH_ROWS, width - keep)
        whole = dot(gate_w[t, 0], got, TN) + dot(gate_w[t, 1], got, TN)
        gate_out[t] = whole.astype(bf16)
        sum_copy(t).start()

    if flood:
        for copy in loads[1:]:
            copy.wait()
        their_weight().start()
        expert([apart + LO * t + lo for t in order], 0)
        for owner in beyond:
            res_copy(owner).wait_recv()
        expert([apart + LO * t + 1 - lo for t in order], 1)
        for owner in (hi, mate):
            res_copy(owner).wait_recv()
        expert([close + j for j in range(take)])
    else:
        repeat(n_sp - 1, lambda k: send_res(k).wait_recv())
        for copy in loads[1:]:
            copy.wait()
        repeat(batches, lambda i: expert([batch_of(i) * take + j for j in range(take)]))
    ret_in[sp] = ret_out[sp]
    y = jnp.concatenate([mix_in[part].astype(f32) for part in range(n_tp)], axis=1)
    hid[...] = hidden_of(y, scaled_v.at[pl.ds(0, rows)], acc, lambda cols: res_ref[:, cols])
    if flood:
        @pl.when(is_gate)
        def _():
            for t in order:
                sum_ready(t)

        others(0, lambda peer: back_copy(peer, peer).wait_recv())
        far_back(lambda peer: back_copy(peer, peer, keep).wait_recv())
        sum_copy(0).wait_recv()
    else:
        repeat(batches, lambda i: others(i, lambda peer: back_copy(peer, peer).wait_recv()))

    def combine(cols):
        got = ret_in[:, :, cols].reshape(slots, 256)
        acc[:, cols] = (
            deep_alpha * hid[:, cols].astype(f32) + dot(w_high, got, TN) + dot(w_low, got, TN)
        )

    def combine_close(cols):
        got = ret_in[pl.ds(close, take), :, pl.ds(cols.start + keep, cols.size)]
        got = got.reshape(BATCH_ROWS, cols.size)
        slab = pl.ds(pl.multiple_of(close * cap, BATCH_ROWS), BATCH_ROWS)
        there = pl.ds(cols.start + keep, cols.size)
        acc[:, there] = (
            deep_alpha * hid[:, there].astype(f32) + sum_in[:, cols].astype(f32)
            + dot(w_out[0, slab, :], got, TN) + dot(w_out[1, slab, :], got, TN)
        )

    every(keep, 256, combine)
    if flood:
        every(width - keep, 256, combine_close)
    o_ref[...] = layer_norm(acc[...], final_gain_ref[...]).astype(bf16)

    for c in sent:
        far_copy(c).wait_send()
    for c in relayed:
        relay_copy(c).wait_send()
    for c in range(PROJ_CHUNKS):
        near_copy(c).wait_send()
    for copy in [proj_near] + mixes:
        copy.wait_send()
    repeat(n_sp - 1, carry_sent)
    if flood:
        repeat(line - 1, lambda k: pick_copy(k).wait_send())
        for part in range(PIECES):
            for kind in range(2):
                raw_copy(kind, part).wait_send()

        @pl.when(is_gate)
        def _():
            for part in range(PIECES):
                for i in range(2):
                    via_copy(i, part).wait_send()

        for owner in range(line):
            res_copy(owner).wait_send()
    else:
        repeat(n_sp - 1, lambda k: send_res(k).wait_send())
    repeat(batches, lambda i: others(i, lambda peer: y_copy(peer, sp).wait_send()))
    if flood:
        others(0, lambda peer: back_copy(peer, sp).wait_send())
        far_back(lambda peer: back_copy(peer, sp, keep).wait_send())
        their_weight().wait_send()
        for t in range(2):
            @pl.when(~is_gate)
            def _():
                part_copy(t, lo, 0).wait_send()

            part_copy(t, 1 - lo, 1).wait_send()

            @pl.when(is_gate)
            def _():
                sum_copy(t).wait_send()
    else:
        repeat(batches, lambda i: others(i, lambda peer: back_copy(peer, sp).wait_send()))


def local(
    mixer_input, retention, decay_real, decay_freq, log_step, input_real, input_imag,
    readout_real, readout_imaginary, skip_weight, norm_gain, projection, residual, mix_gain,
    routes, route_weight, expert_gate, expert_up, expert_down, final_gain,
):
    n_sp, n_tp = lax.axis_size("sp"), lax.axis_size("tp")
    tokens, chans = mixer_input.shape
    groups, states, channels = input_real.shape
    gp, rows, width = groups * states, residual.shape[0], residual.shape[1]
    cap = -(-max(2, 2 * rows * PICKS // n_sp) // 16) * 16
    hidden, line = expert_gate.shape[2], n_sp // LO
    take = BATCH_ROWS // cap
    rest = width - width // DIRECT_SHARE if n_sp == 8 else 128

    def compact(value):
        return jnp.swapaxes(value, 1, 2).reshape(chans, states)

    small = (
        mixer_input, retention, decay_real, decay_freq, log_step[None, :], skip_weight,
        norm_gain[None, :], compact(input_real), compact(input_imag),
        readout_real.reshape(chans, states), readout_imaginary.reshape(chans, states),
        residual, mix_gain[None, :], routes.T, route_weight.T, final_gain[None, :],
    )
    vmem = pl.BlockSpec(memory_space=pltpu.VMEM)
    anywhere = pl.BlockSpec(memory_space=pl.ANY)
    dma = pltpu.SemaphoreType.DMA
    return pl.pallas_call(
        functools.partial(kernel, n_sp, n_tp, groups, channels, states, cap),
        out_shape=jax.ShapeDtypeStruct((rows, width), bf16),
        in_specs=[anywhere] * (len(small) + 4),
        out_specs=vmem,
        scratch_shapes=[pltpu.VMEM(value.shape, value.dtype) for value in small]
        + [
            pltpu.VMEM((tokens, gp), f32),
            pltpu.VMEM((tokens, gp), f32),
            pltpu.VMEM((tokens, gp), f32),
            pltpu.VMEM((3, gp), f32),
            pltpu.VMEM((n_sp, 3, gp), f32),
            pltpu.VMEM((tokens, chans), bf16),
            pltpu.VMEM((n_tp, rows, chans), bf16),
            pltpu.VMEM((n_tp,) + projection.shape, bf16),
            pltpu.VMEM((width, hidden), bf16),
            pltpu.VMEM((width, hidden), bf16),
            pltpu.VMEM((hidden, width), bf16),
            pltpu.VMEM((rows, width), f32),
            pltpu.VMEM((rows, width), bf16),
            pltpu.VMEM((BATCH_ROWS, n_tp * chans), bf16),
            pltpu.VMEM((BATCH_ROWS, width), f32),
            pltpu.VMEM((BATCH_ROWS, width), bf16),
            pltpu.VMEM((n_sp * cap, rows), bf16),
            pltpu.VMEM((line, LO * cap, rows), bf16),
            pltpu.VMEM((line, rows, width) if n_sp == 8 else (1, 16, 128), bf16),
            pltpu.VMEM((n_sp, cap, width), bf16),
            pltpu.VMEM((n_sp, cap, width), bf16),
            pltpu.VMEM((n_sp, cap, n_tp * chans), bf16),
            pltpu.VMEM((n_sp, cap, n_tp * chans), bf16),
            pltpu.VMEM((n_sp, cap, width), bf16),
            pltpu.VMEM((n_sp, cap, width), bf16),
            pltpu.VMEM((2, n_sp * cap, rows), bf16),
            pltpu.VMEM((2, 2, take * cap, rows), bf16),
            pltpu.VMEM((2, take, cap, rest), bf16),
            pltpu.VMEM((2, rows, rest), bf16),
            pltpu.VMEM((rows, rest), bf16),
            dma((len(small),)), dma((4,)),
            dma((n_sp,)), dma((n_sp,)),
            dma((n_tp,)), dma((n_tp,)),
            dma((PROJ_CHUNKS + 1,)), dma((PROJ_CHUNKS + 1,)),
            dma((PROJ_CHUNKS,)), dma((PROJ_CHUNKS,)),
            dma((PROJ_CHUNKS,)), dma((line,)), dma((line,)),
            dma((2 * PIECES,)), dma((line * PIECES,)), dma((2 * PIECES,)),
            dma((n_sp,)), dma((n_sp,)),
            dma((n_sp,)), dma((n_sp,)),
            dma((n_sp,)), dma((n_sp,)),
            dma((1,)), dma((2,)), dma((4,)), dma((2 * take,)), dma((2,)), dma((1,)),
        ],
        compiler_params=pltpu.CompilerParams(
            collective_id=0, has_side_effects=True, vmem_limit_bytes=60 * 1024 * 1024
        ),
    )(
        *small,
        projection, expert_gate, expert_up, expert_down,
    )


def solution(mesh):
    in_specs = (
        P("sp", "tp"),
        P("tp", "sp"),
        P("tp", None),
        P("tp", None),
        P("tp"),
        P("tp", None, None),
        P("tp", None, None),
        P("tp", None, None),
        P("tp", None, None),
        P("tp", None),
        P(),
        P("tp", None),
        P(("sp", "tp"), None),
        P(),
        P(("sp", "tp"), None),
        P(("sp", "tp"), None),
        P("sp", None, None),
        P("sp", None, None),
        P("sp", None, None),
        P(),
    )
    out_specs = P(("sp", "tp"), None)
    return jax.shard_map(local, mesh=mesh, in_specs=in_specs, out_specs=out_specs, check_vma=False)
```
